32 devices in a mesh: ep: 8 (over z, core), tp: 4 (over y, x).
Axes of the slice: x: 2, y: 2, z: 4, core: 2. Of those that a mesh axis runs over, the one named last changes fastest.
Arguments:
- query_proj: bfloat16 [4096, 1024], P('ep', 'tp'), may hold values from -6 to 6
- key_proj: bfloat16 [4096, 256], P('ep'), may hold values from -6 to 6
- value_proj: bfloat16 [4096, 256], P('ep'), may hold values from -24 to 24
- sink_logit: float32 [16], P('tp'), may hold values from 2 to 6
- out_weight: bfloat16 [1024, 2048], P(None, 'tp'), may hold values from -0.1875 to 0.1875
- expert_input: bfloat16 [2048, 2048], P('ep'), may hold values from -6 to 6
- norm_gain: float32 [2048], replicated, may hold values from 0.1 to 1.9
- routes: int32 [2048, 2], P('ep'), may hold values from 0 to 7, as said below
- route_weights: float32 [2048, 2], P('ep'), may hold values from 0.2 to 1
- gate_weight: bfloat16 [8, 2048, 4096], P('ep', None, 'tp'), may hold values from -0.125 to 0.125
- up_weight: bfloat16 [8, 2048, 4096], P('ep', None, 'tp'), may hold values from -0.125 to 0.125
- down_weight: bfloat16 [8, 4096, 2048], P('ep', 'tp'), may hold values from -0.09375 to 0.09375
Outputs:
- mixer_out: bfloat16 [4096, 2048], P('ep', 'tp')
- expert_out: bfloat16 [2048, 2048], P('ep', 'tp')
The draws below stay inside these ranges and needn't reach their ends.
Inputs may be any that keep to these rules, and one draw needn't show every extreme that they name: `routes`: experts form 4 groups of consecutive numbers of equal size. Each row names 2 different experts of one group. In each aligned block of 256 rows no expert is named by more than 128 rows, and in every block some expert is named by exactly 128 rows.
All inputs are finite; a program needn't handle non-finite values.
Results may differ from the reference program's by a relative error of at most 0.017.
Values may be sent and summed in bfloat16 or wider, within the bound.
A program may use at most 64 MiB of HBM per device.

```python
import jax
import jax.numpy as jnp
from jax import lax

D = 2048
HEADS = 16
KV_HEADS = 4
HEAD_DIM = 64
HALF_WIN = 128
ROWS_B = 256
TOK_A = 4096
TOK_B = 2048
EXPERTS = 8
GROUPS = 4
TOP_K = 2
EXP_HID = 4096
CAP = 128
N_TP = 4


def drawn_pair(key):
    base_key = jax.random.fold_in(key, 7)
    key_rows = jax.random.normal(jax.random.fold_in(base_key, 1), (TOK_A, KV_HEADS * HEAD_DIM), jnp.float32)
    query_rows = jax.random.normal(jax.random.fold_in(base_key, 2), (TOK_A, HEADS * HEAD_DIM), jnp.float32)
    return (jnp.clip(query_rows, -6.0, 6.0), jnp.clip(key_rows, -6.0, 6.0))


def draw_query_proj(key, part):
    return drawn_pair(key)[0].astype(jnp.bfloat16)


def draw_key_proj(key, part):
    return drawn_pair(key)[1].astype(jnp.bfloat16)


def draw_routes(key, part):
    per_group = EXPERTS // GROUPS
    block_count = TOK_B // ROWS_B
    base_key = jax.random.fold_in(key, 31)
    busy_group = jax.random.randint(jax.random.fold_in(base_key, 1), (block_count, 1), 0, GROUPS)
    other_step = jax.random.randint(jax.random.fold_in(base_key, 2), (block_count, ROWS_B), 1, GROUPS)
    order_keys = jax.random.split(jax.random.fold_in(base_key, 3), block_count)
    row_order = jax.vmap(lambda sub_key: jax.random.permutation(sub_key, ROWS_B))(order_keys)
    in_busy = row_order < ROWS_B // 2
    group_ids = jnp.where(in_busy, busy_group, (busy_group + other_step) % GROUPS)
    onehot = (group_ids[:, :, None] == jnp.arange(GROUPS, dtype=jnp.int32)[None, None, :]).astype(jnp.int32)
    group_rank = jnp.sum((jnp.cumsum(onehot, axis=1) - onehot) * onehot, axis=2)
    offsets = jax.random.randint(jax.random.fold_in(base_key, 4), (block_count, GROUPS), 0, per_group)
    shifts = jax.random.randint(jax.random.fold_in(base_key, 5), (block_count, GROUPS), 1, per_group)
    offset_row = jnp.take_along_axis(offsets, group_ids, axis=1)
    shift_row = jnp.take_along_axis(shifts, group_ids, axis=1)
    first_pick = (group_rank + offset_row) % per_group
    second_pick = (group_rank + offset_row + shift_row) % per_group
    chosen = group_ids[:, :, None] * per_group + jnp.stack([first_pick, second_pick], axis=-1)
    return chosen.reshape(TOK_B, TOP_K).astype(jnp.int32)


def block_levels(stream_key, dims, cuts, low, top_value):
    loudness = 1.0
    for axis_at, blocks in cuts:
        draws = jax.random.uniform(jax.random.fold_in(jax.random.fold_in(stream_key, 6), axis_at), (blocks,), jnp.float32, low / len(cuts), top_value / len(cuts))
        loudness = loudness * jnp.repeat(jnp.exp(draws), dims[axis_at] // blocks).reshape((-1,) + (1,) * (len(dims) - 1 - axis_at))
    return loudness


def centred(own_key, extent, spread, bound, cuts=(), held_as=jnp.bfloat16):
    result = spread * jax.random.normal(own_key, extent, jnp.float32)
    if cuts:
        result = result * block_levels(own_key, extent, cuts, -0.22, 0.18)
    return jnp.clip(result, -bound, bound).astype(held_as)


def setup_inputs(seed: int = 0) -> dict:
    splits = jax.random.split(jax.random.key(seed), 13)
    query_proj = draw_query_proj(jax.random.fold_in(splits[12], 71), 0)
    key_proj = draw_key_proj(jax.random.fold_in(splits[12], 71), 0)
    value_proj = centred(splits[2], (TOK_A, KV_HEADS * HEAD_DIM), 4.0, 24.0, ((0, 8),))
    sink_logit = jnp.clip(2.0 + 4.0 * jax.random.uniform(splits[3], (HEADS,), jnp.float32) ** block_levels(splits[3], (HEADS,), ((0, 4),), -0.2, 0.2), 2.0, 6.0)
    out_weight = centred(splits[4], (HEADS * HEAD_DIM, D), (HEADS * HEAD_DIM) ** -0.5, 0.1875, ((1, 4),))
    expert_input = centred(splits[5], (TOK_B, D), 1.0, 6.0, ((0, 8),))
    norm_gain = jnp.clip(1.0 + 0.18 * jax.random.normal(splits[6], (D,), jnp.float32), 0.1, 1.9)
    routes = draw_routes(jax.random.fold_in(splits[12], 71), 0)
    route_weights = jnp.clip(0.2 + 0.8 * jax.random.uniform(splits[8], (TOK_B, TOP_K), jnp.float32) ** block_levels(splits[8], (TOK_B, TOP_K), ((0, 8),), -0.2, 0.2), 0.2, 1.0)
    gate_weight = centred(splits[9], (EXPERTS, D, EXP_HID), D ** -0.5, 0.125, ((0, 8), (2, 4)))
    up_weight = centred(splits[10], (EXPERTS, D, EXP_HID), D ** -0.5, 0.125, ((0, 8), (2, 4)))
    down_weight = centred(splits[11], (EXPERTS, EXP_HID, D), EXP_HID ** -0.5, 0.09375, ((0, 8), (1, 4)))
    return dict(query_proj=query_proj, key_proj=key_proj, value_proj=value_proj, sink_logit=sink_logit, out_weight=out_weight, expert_input=expert_input, norm_gain=norm_gain, routes=routes, route_weights=route_weights, gate_weight=gate_weight, up_weight=up_weight, down_weight=down_weight)


NORM_EPS = 1e-06
ROPE_BASE = 10000.0
NEG_BIG = -1e+30

def rotate(features, position_start):
    count = features.shape[0]
    half_dim = features.shape[-1] // 2
    inverse_freq = 1.0 / ROPE_BASE ** (jnp.arange(half_dim, dtype=jnp.float32) * 2.0 / features.shape[-1])
    position = (jnp.arange(count, dtype=jnp.int32) + position_start).astype(jnp.float32)
    angles = position[:, None] * inverse_freq[None, :]
    cosine = jnp.cos(angles)[:, None, :]
    sine_part = jnp.sin(angles)[:, None, :]
    lower_half = features[..., :half_dim]
    upper_half = features[..., half_dim:]
    return jnp.concatenate([lower_half * cosine - upper_half * sine_part, upper_half * cosine + lower_half * sine_part], axis=-1)

def attention_ref(query_proj, key_proj, value_proj, sink_logit):
    seq_total = query_proj.shape[0]
    per_kv = HEADS // KV_HEADS
    rot_q = rotate(query_proj.reshape(seq_total, HEADS, HEAD_DIM).astype(jnp.float32), 0).astype(jnp.bfloat16)
    rot_k = rotate(key_proj.reshape(seq_total, KV_HEADS, HEAD_DIM).astype(jnp.float32), 0).astype(jnp.bfloat16)
    padding = ((HALF_WIN, HALF_WIN), (0, 0), (0, 0))
    padded_k = jnp.pad(rot_k, padding)
    padded_v = jnp.pad(value_proj.reshape(seq_total, KV_HEADS, HEAD_DIM), padding)
    grouped_sink = sink_logit.reshape(KV_HEADS, per_kv)
    block_rows = min(512, seq_total)
    key_rows = block_rows + 2 * HALF_WIN

    def one_block(block_index):
        start_row = block_index * block_rows
        query_block = lax.dynamic_slice_in_dim(rot_q, start_row, block_rows, 0).reshape(block_rows, KV_HEADS, per_kv, HEAD_DIM).astype(jnp.float32)
        key_block = lax.dynamic_slice_in_dim(padded_k, start_row, key_rows, 0).astype(jnp.float32)
        value_block = lax.dynamic_slice_in_dim(padded_v, start_row, key_rows, 0).astype(jnp.float32)
        scores = jnp.einsum('qngd,knd->ngqk', query_block, key_block) * HEAD_DIM ** (-0.5)
        key_offset = jnp.arange(key_rows, dtype=jnp.int32) - HALF_WIN
        key_gap = key_offset[None, :] - jnp.arange(block_rows, dtype=jnp.int32)[:, None]
        global_key = start_row + key_offset
        allowed = (jnp.abs(key_gap) <= HALF_WIN) & (global_key >= 0)[None, :] & (global_key < seq_total)[None, :]
        scores = jnp.where(allowed[None, None], scores, NEG_BIG)
        row_peak = jnp.maximum(lax.optimization_barrier(jnp.max(scores, axis=-1)), grouped_sink[:, :, None])
        lifted = jnp.exp(scores - row_peak[..., None])
        norm_total = lax.optimization_barrier(jnp.sum(lifted, axis=-1)) + jnp.exp(grouped_sink[:, :, None] - row_peak)
        probs = (lifted / norm_total[..., None]).astype(jnp.bfloat16)
        weighted = jnp.einsum('ngqk,knd->qngd', probs.astype(jnp.float32), value_block)
        return weighted.astype(jnp.bfloat16).reshape(block_rows, HEADS * HEAD_DIM)
    blocks = lax.map(one_block, jnp.arange(seq_total // block_rows, dtype=jnp.int32))
    return blocks.reshape(seq_total, HEADS * HEAD_DIM)

def experts_ref(expert_input, norm_gain, routes, route_weights, gate_weight, up_weight, down_weight):
    widened = expert_input.astype(jnp.float32)
    normed = (widened * lax.rsqrt(lax.optimization_barrier(jnp.mean(widened * widened, axis=1, keepdims=True)) + NORM_EPS) * norm_gain).astype(jnp.bfloat16)
    block_count = TOK_B // ROWS_B
    flat_routes = routes.reshape(block_count, ROWS_B * TOP_K)
    onehot = (flat_routes[:, :, None] == jnp.arange(EXPERTS, dtype=jnp.int32)[None, None, :]).astype(jnp.int32)
    slot_rank = lax.optimization_barrier(jnp.sum((jnp.cumsum(onehot, axis=1) - onehot) * onehot, axis=2))
    row_index = (jnp.arange(TOK_B * TOP_K, dtype=jnp.int32) // TOP_K).reshape(block_count, ROWS_B * TOP_K)
    block_index = jnp.broadcast_to(jnp.arange(block_count, dtype=jnp.int32)[:, None], flat_routes.shape)
    table = jnp.zeros((EXPERTS, block_count, CAP), jnp.int32).at[flat_routes, block_index, slot_rank].set(row_index)
    span_units = EXP_HID // N_TP

    def one_expert(operands):
        rows_table, gate_x, up_x, down_x = operands
        gathered = normed[rows_table.reshape(-1)]
        gate_sum = jnp.dot(gathered, gate_x, preferred_element_type=jnp.float32)
        up_sum = jnp.dot(gathered, up_x, preferred_element_type=jnp.float32)
        hidden = (jax.nn.silu(gate_sum) * up_sum).astype(jnp.bfloat16)
        slot_total = hidden.shape[0]
        parts = jnp.einsum('snh,nhd->nsd', hidden.reshape(slot_total, N_TP, span_units).astype(jnp.float32), down_x.reshape(N_TP, span_units, D).astype(jnp.float32)).astype(jnp.bfloat16)
        return lax.optimization_barrier(jnp.sum(parts.astype(jnp.float32), axis=0)).astype(jnp.bfloat16)
    results = lax.map(one_expert, (table, gate_weight, up_weight, down_weight))
    picked = results[flat_routes, block_index * CAP + slot_rank]
    picked = picked.reshape(TOK_B, TOP_K, D).astype(jnp.float32)
    return lax.optimization_barrier(jnp.sum(picked * route_weights[:, :, None], axis=1)).astype(jnp.bfloat16)

def reference(query_proj, key_proj, value_proj, sink_logit, out_weight, expert_input, norm_gain, routes, route_weights, gate_weight, up_weight, down_weight):
    attended = attention_ref(query_proj, key_proj, value_proj, sink_logit)
    mixer_out = jnp.dot(attended, out_weight, preferred_element_type=jnp.float32).astype(jnp.bfloat16)
    expert_out = experts_ref(expert_input, norm_gain, routes, route_weights, gate_weight, up_weight, down_weight)
    return (mixer_out, expert_out)
```

```python
import jax
import jax.numpy as jnp
import numpy as np
from jax import lax
from jax.experimental import pallas as pl
from jax.experimental.pallas import tpu as pltpu
from jax.sharding import PartitionSpec as P

D = 2048
HEADS = 16
KV_HEADS = 4
HEAD_DIM = 64
HALF_WIN = 128
GROUPS = 4
TOP_K = 2


NORM_EPS = 1e-06
ROPE_BASE = 10000.0
NEG_BIG = -1e30
MESH = pl.DeviceIdType.MESH
SIDE = 128


def padded(block, sides, width):
    for axis, dim in sides:
        count = lax.axis_size(axis)
        forward = [(i, i + 1) for i in range(count - 1)]
        backward = [(target, source) for source, target in forward]
        low = lax.ppermute(
            lax.slice_in_dim(block, block.shape[dim] - width, None, axis=dim), axis, forward
        )
        high = lax.ppermute(lax.slice_in_dim(block, 0, width, axis=dim), axis, backward)
        block = jnp.concatenate([low, block, high], axis=dim)
    return block


def rotate(features, position_start):
    count = features.shape[0]
    half_dim = features.shape[-1] // 2
    inverse_freq = 1.0 / ROPE_BASE ** (
        jnp.arange(half_dim, dtype=jnp.float32) * 2.0 / features.shape[-1]
    )
    position = (jnp.arange(count, dtype=jnp.int32) + position_start).astype(jnp.float32)
    angles = position[:, None] * inverse_freq[None, :]
    cosine = jnp.cos(angles)[:, None, :]
    sine_part = jnp.sin(angles)[:, None, :]
    lower_half = features[..., :half_dim]
    upper_half = features[..., half_dim:]
    return jnp.concatenate(
        [
            lower_half * cosine - upper_half * sine_part,
            upper_half * cosine + lower_half * sine_part,
        ],
        axis=-1,
    )


def mixer_half(query_proj, key_proj, value_proj, sink_logit, out_weight):
    row_count = query_proj.shape[0]
    local_heads = query_proj.shape[1] // HEAD_DIM
    per_kv = HEADS // KV_HEADS
    kv_local = max(1, local_heads // per_kv)
    group_size = local_heads // kv_local
    tp_index = lax.axis_index("tp")
    offset = lax.axis_index("ep") * row_count
    seq_total = row_count * lax.axis_size("ep")
    first_kv = tp_index * local_heads // per_kv
    own_keys = lax.dynamic_slice_in_dim(key_proj, first_kv * HEAD_DIM, kv_local * HEAD_DIM, 1)
    own_values = lax.dynamic_slice_in_dim(value_proj, first_kv * HEAD_DIM, kv_local * HEAD_DIM, 1)
    rot_q = rotate(
        query_proj.reshape(row_count, local_heads, HEAD_DIM).astype(jnp.float32), offset
    ).astype(jnp.bfloat16)
    rot_k = rotate(
        own_keys.reshape(row_count, kv_local, HEAD_DIM).astype(jnp.float32), offset
    ).astype(jnp.bfloat16)
    stacked = jnp.stack([rot_k, own_values.reshape(row_count, kv_local, HEAD_DIM)])
    extended = padded(stacked, (("ep", 1),), HALF_WIN)
    own_sink = sink_logit.reshape(kv_local, group_size)
    block_rows = min(512, row_count)
    key_rows = block_rows + 2 * HALF_WIN
    key_offset = jnp.arange(key_rows, dtype=jnp.int32) - HALF_WIN
    key_gap = key_offset[None, :] - jnp.arange(block_rows, dtype=jnp.int32)[:, None]
    query_block = rot_q.reshape(block_rows, kv_local, group_size, HEAD_DIM)
    key_block = extended[0, 0:key_rows]
    value_block = extended[1, 0:key_rows]
    scores = jnp.einsum(
        "qngd,knd->ngqk", query_block, key_block, preferred_element_type=jnp.float32
    ) * HEAD_DIM ** (-0.5)
    global_key = offset + 0 + key_offset
    allowed = (
        (jnp.abs(key_gap) <= HALF_WIN)
        & (global_key >= 0)[None, :]
        & (global_key < seq_total)[None, :]
    )
    scores = jnp.where(allowed[None, None], scores, NEG_BIG)
    row_peak = jnp.maximum(jnp.max(scores, axis=-1), own_sink[:, :, None])
    lifted = jnp.exp(scores - row_peak[..., None])
    norm_total = jnp.sum(lifted, axis=-1) + jnp.exp(own_sink[:, :, None] - row_peak)
    probs = (lifted / norm_total[..., None]).astype(jnp.bfloat16)
    weighted = jnp.einsum("ngqk,knd->qngd", probs, value_block, preferred_element_type=jnp.float32)
    pieces = weighted.astype(jnp.bfloat16).reshape(block_rows, local_heads * HEAD_DIM)
    projected = jnp.dot(
        lax.all_gather(pieces, "tp", axis=1, tiled=True),
        out_weight,
        preferred_element_type=jnp.float32,
    )
    return projected.astype(jnp.bfloat16)


def expert_half(
    expert_input, norm_gain, routes, route_weights, gate_weight, up_weight, down_weight
):
    row_count = expert_input.shape[0]
    widened = expert_input.astype(jnp.float32)
    normed = (
        widened
        * lax.rsqrt(jnp.mean(widened * widened, axis=1, keepdims=True) + NORM_EPS)
        * norm_gain
    ).astype(jnp.bfloat16)
    local_experts = gate_weight.shape[0]
    ep_count = lax.axis_size("ep")
    expert_count = local_experts * ep_count
    capacity = row_count * GROUPS // expert_count
    col_count = D // lax.axis_size("tp")
    flat_routes = routes.reshape(-1)
    onehot = (flat_routes[:, None] == jnp.arange(expert_count, dtype=jnp.int32)[None, :]).astype(
        jnp.int32
    )
    slot_rank = jnp.sum((jnp.cumsum(onehot, axis=0) - onehot) * onehot, axis=1)
    slot_index = flat_routes * capacity + slot_rank
    source_rows = jnp.arange(row_count * TOP_K, dtype=jnp.int32) // TOP_K
    own_cols = lax.dynamic_slice_in_dim(normed, lax.axis_index("tp") * col_count, col_count, 1)
    outgoing = (
        jnp.zeros((expert_count * capacity, col_count), jnp.bfloat16)
        .at[slot_index]
        .set(own_cols[source_rows])
    )
    arrived = lax.all_to_all(
        outgoing.reshape(expert_count, capacity, col_count),
        "ep",
        split_axis=0,
        concat_axis=1,
        tiled=True,
    )
    shard_piece = lax.all_gather(arrived, "tp", axis=2, tiled=True)
    gate_sum = jnp.einsum(
        "esd,edh->esh", shard_piece, gate_weight, preferred_element_type=jnp.float32
    )
    up_sum = jnp.einsum("esd,edh->esh", shard_piece, up_weight, preferred_element_type=jnp.float32)
    hidden = (jax.nn.silu(gate_sum) * up_sum).astype(jnp.bfloat16)
    slot_total = hidden.shape[1]
    term = jnp.einsum("esh,ehc->ces", hidden, down_weight, preferred_element_type=jnp.float32)
    summed = lax.psum_scatter(
        term.reshape(col_count * lax.axis_size("tp"), local_experts * slot_total).astype(
            jnp.bfloat16
        ),
        "tp",
        scatter_dimension=0,
        tiled=True,
    )
    result = summed.reshape(col_count, local_experts, ep_count, capacity)
    returned = lax.all_to_all(result, "ep", split_axis=2, concat_axis=1, tiled=True)
    returned = returned.reshape(col_count, expert_count * capacity)
    picked = (
        jnp.take(returned, slot_index, axis=1)
        .reshape(col_count, row_count, TOP_K)
        .astype(jnp.float32)
    )
    combined = jnp.sum(picked * route_weights[None, :, :], axis=2)
    return combined.T.astype(jnp.bfloat16)


def local(
    query_proj,
    key_proj,
    value_proj,
    sink_logit,
    out_weight,
    expert_input,
    norm_gain,
    routes,
    route_weights,
    gate_weight,
    up_weight,
    down_weight,
):
    mixer_out = mixer_half(query_proj, key_proj, value_proj, sink_logit, out_weight)
    expert_out = expert_half(
        expert_input, norm_gain, routes, route_weights, gate_weight, up_weight, down_weight
    )
    return (mixer_out, expert_out)


def fits_fused(mesh):
    return (
        mesh.shape["tp"] == 4
        and mesh.shape["ep"] == 2 * GROUPS
        and HALF_WIN == SIDE
        and HEADS // KV_HEADS == 4
        and KV_HEADS == 4
    )


class Slots:
    def __init__(self):
        self.names = {}

    def __call__(self, *name):
        return self.names.setdefault(name, len(self.names))


RECV_SLOTS = 39
SEND_SLOTS = 14


def fused_kernel(
    x_hbm, routes_hbm, rw_hbm, gain_hbm, key_hbm, value_hbm, q_hbm, table_hbm, sink_hbm,
    wg_hbm, wu_hbm, wd_hbm, wout_hbm,
    mixer_ref, expert_ref,
    x_ref, routes_ref, rw_ref, gain_ref, key_ref, value_ref, q_ref, table_ref, sink_ref,
    wg, wu, wd, wout,
    kve, krot, att, sel_ret, snd, xs, wgt, hid, yb, yr, zs, rx, ry, sb, r2, fin, ret, acc,
    ssem, rsem, wsem,
):
    ep = lax.axis_index("ep")
    t = lax.axis_index("tp")
    chips = GROUPS
    z, core = ep // 2, ep % 2
    partner = ep + 1 - 2 * core
    other = (ep + 2 * core - 1 + 2 * chips) % (2 * chips)
    up, down = (ep + 1) % (2 * chips), (ep + 2 * chips - 1) % (2 * chips)
    ty, tx = t // 2, t % 2
    t_x, t_y, t_d = ty * 2 + 1 - tx, (1 - ty) * 2 + tx, (1 - ty) * 2 + 1 - tx
    rows = q_ref.shape[0]
    tokens, model = x_ref.shape
    cap = xs.shape[1] // 2
    part = cap // 4
    half_part, half_cap = part // 2, cap // 2
    hidden = wg.shape[1]
    cols = wout.shape[1]
    slots, send_slots = Slots(), Slots()
    z_of = (z, z + 1 - 2 * (z % 2), (z + 2) % chips, chips - 1 - z)

    def remote(send_index, recv_index, src, dst, device):
        return pltpu.make_async_remote_copy(
            src_ref=src, dst_ref=dst, send_sem=ssem.at[send_index], recv_sem=rsem.at[recv_index],
            device_id=device, device_id_type=MESH,
        )

    def send(family, name, src, dst, device):
        remote(send_slots(family), slots(*name), src, dst, device).start()

    def arrive(name, dst):
        remote(0, slots(*name), dst, dst, (ep, t_x)).wait_recv()

    def sent(family, src):
        remote(send_slots(family), 0, src, src, (ep, t_x)).wait_send()

    barrier = pltpu.get_barrier_semaphore()
    peers = [(z_of[k] * 2 + core, t) for k in range(1, chips)]
    peers += [(ep, t_x), (ep, t_y), (partner, t), (other, t)]
    for peer in peers:
        pl.semaphore_signal(barrier, inc=1, device_id=peer, device_id_type=MESH)

    pairs = (
        (x_hbm, x_ref), (routes_hbm, routes_ref), (rw_hbm, rw_ref), (gain_hbm, gain_ref),
        (key_hbm, key_ref), (value_hbm, value_ref), (q_hbm, q_ref), (table_hbm, table_ref),
        (sink_hbm, sink_ref), (wg_hbm, wg), (wu_hbm, wu), (wd_hbm, wd), (wout_hbm, wout),
    )
    order = (0, 1, 2, 3, 4, 4, 4, 5, 6, 7, 8, 9, 10)
    loads = [pltpu.make_async_copy(a, b, wsem.at[i]) for i, (a, b) in zip(order, pairs)]
    for copy in loads[:9]:
        copy.start()
    for copy in loads[:4]:
        copy.wait()
    for copy in loads[9:]:
        copy.start()

    wide = x_ref[...].astype(jnp.float32)
    inverse = lax.rsqrt(jnp.mean(wide * wide, axis=1, keepdims=True) + NORM_EPS)
    normed = (wide * inverse * gain_ref[...]).astype(jnp.bfloat16)
    group = routes_ref[0:1, :] >> 1
    row_i = lax.broadcasted_iota(jnp.int32, (tokens, tokens), 0)
    col_i = lax.broadcasted_iota(jnp.int32, (tokens, tokens), 1)
    later = jnp.where(row_i < col_i, 1.0, 0.0).astype(jnp.bfloat16)
    hot = jnp.where(lax.broadcasted_iota(jnp.int32, (16, tokens), 0) == group, 1.0, 0.0)
    count = jnp.dot(hot.astype(jnp.bfloat16), later, preferred_element_type=jnp.float32)
    rank = jnp.sum(count * hot, axis=0, keepdims=True).astype(jnp.int32)

    odd = (routes_ref[...] & 1) == 1
    weight_odd = jnp.sum(jnp.where(odd, rw_ref[...], 0.0), axis=0, keepdims=True)
    weight_even = jnp.sum(jnp.where(odd, 0.0, rw_ref[...]), axis=0, keepdims=True)
    lane = lax.broadcasted_iota(jnp.int32, (128, tokens), 0)
    weight = jnp.where(lane < 2, weight_even, weight_odd)
    high = weight.astype(jnp.bfloat16).astype(jnp.float32)
    weight = jnp.where((lane & 1) == 0, high, weight - high)
    weight = jnp.where(lane < 4, weight, 0.0).astype(jnp.bfloat16)

    def select(pick, out, at):
        pick = jnp.where(pick, 1.0, 0.0).astype(jnp.bfloat16)
        out[at, model:] = lax.dot_general(
            pick, weight, (((1,), (1,)), ((), ())), preferred_element_type=jnp.float32
        ).astype(jnp.bfloat16)
        out[at, :model] = jnp.dot(pick, normed, preferred_element_type=jnp.float32).astype(
            jnp.bfloat16
        )

    def group_at(index):
        return jnp.where(
            index == 0, z_of[0],
            jnp.where(index == 1, z_of[1], jnp.where(index == 2, z_of[2], z_of[3])),
        )

    slot = lax.broadcasted_iota(jnp.int32, (chips * part, tokens), 0)
    index = slot // part
    owner = jnp.where(index == 1, t_d, t)
    select(
        (group == group_at(jnp.maximum(index, 1)))
        & (rank == owner * part + lax.rem(slot, part)),
        snd, slice(0, chips * part),
    )

    def piece(k, owner_t, start=0, count=part):
        first = pl.multiple_of(core * cap + owner_t * part + start, 16)
        return xs.at[k, pl.ds(first, count)]

    def own_rows(k, which):
        return xs.at[k, pl.ds(pl.multiple_of(which * cap, 16), cap)]

    pltpu.make_async_copy(att.at[pl.ds(0, 3)], att.at[pl.ds(0, 3)], wsem.at[4]).wait()
    for copy in loads[7:9]:
        copy.wait()
    row_i = lax.broadcasted_iota(jnp.int32, (key_ref.shape[1], 2 * HEAD_DIM), 0)
    col_i = lax.broadcasted_iota(jnp.int32, (key_ref.shape[1], 2 * HEAD_DIM), 1)
    own_key = jnp.where((row_i == t * HEAD_DIM + col_i) & (col_i < HEAD_DIM), 1.0, 0.0)
    own_value = jnp.where(
        (row_i == (t - 1) * HEAD_DIM + col_i) & (col_i >= HEAD_DIM), 1.0, 0.0
    )
    both = jnp.dot(
        key_ref[...], own_key.astype(jnp.bfloat16), preferred_element_type=jnp.float32
    ) + jnp.dot(
        value_ref[...], own_value.astype(jnp.bfloat16), preferred_element_type=jnp.float32
    )
    kve[SIDE : SIDE + rows, :] = both.astype(jnp.bfloat16)

    pl.semaphore_wait(barrier, len(peers))
    send("halo", ("halo",), kve.at[pl.ds(rows, SIDE)], kve.at[pl.ds(0, SIDE)], (up, t))
    send("halo", ("halo",), kve.at[pl.ds(SIDE, SIDE)], kve.at[pl.ds(SIDE + rows, SIDE)], (down, t))
    for i, (k, owner_t, name) in enumerate(
        ((1, t, "z"), (1, t_d, "s"), (2, t, "z"), (3, t, "z"))
    ):
        send(
            "z", (name, k), snd.at[pl.ds(i * part, part)], piece(k, owner_t),
            (z_of[k] * 2 + core, t),
        )

    slot = lax.broadcasted_iota(jnp.int32, (cap, tokens), 0)
    select(
        (group == z) & (rank == slot), xs.at[0], pl.ds(pl.multiple_of(core * cap, 16), cap)
    )
    send("p", ("p", 0), own_rows(0, core), own_rows(0, core), (partner, t))

    def select_back():
        slot = lax.broadcasted_iota(jnp.int32, (chips * cap, tokens), 0)
        place = (group == group_at(slot // cap)) & (rank == lax.rem(slot, cap))
        sel_ret[...] = jnp.where(place, 1.0, 0.0).T.astype(jnp.bfloat16)

    def spread(k):
        arrive(("z", k), piece(k, t))
        if k == 1:
            send("x", ("s", k), piece(k, t), piece(k, t), (ep, t_x))
            send("y", ("s", k), piece(k, t), piece(k, t), (ep, t_y))
            return
        for family, name, start, device in (
            ("x", "xl", 0, t_x), ("y", "yh", half_part, t_y),
            ("x", "s", half_part, t_x), ("y", "s", 0, t_y),
        ):
            rows_of = piece(k, t, start, half_part)
            send(family, (name, k), rows_of, rows_of, (ep, device))

    def relay(k):
        arrive(("xl", k), piece(k, t_x, 0, half_part))
        rows_of = piece(k, t_x, 0, half_part)
        send("d", ("s", k), rows_of, rows_of, (ep, t_y))
        arrive(("yh", k), piece(k, t_y, half_part, half_part))
        rows_of = piece(k, t_y, half_part, half_part)
        send("d", ("s", k), rows_of, rows_of, (ep, t_x))

    def share(k):
        arrive(("s", k), snd.at[pl.ds(0, (3 if k == 1 else 2) * part)])
        send("p", ("p", k), own_rows(k, core), own_rows(k, core), (partner, t))

    def swap_matrix(size):
        i = lax.broadcasted_iota(jnp.int32, (size, size), 0)
        j = lax.broadcasted_iota(jnp.int32, (size, size), 1)
        half = HEAD_DIM // 2
        low = (j & (HEAD_DIM - 1)) < half
        minus = low & (i == j + half)
        plus = (~low) & (i == j - half)
        return jnp.where(minus, -1.0, jnp.where(plus, 1.0, 0.0)).astype(jnp.bfloat16)

    blocks = rows // SIDE
    far_rows = (table_ref.shape[0] - 2 * SIDE) // 2

    def tables(block):
        at = ep * blocks + block
        far_c = table_ref[pl.ds(at, 1), :]
        far_s = table_ref[pl.ds(far_rows + at, 1), :]
        near_c = table_ref[2 * far_rows : 2 * far_rows + SIDE, :]
        near_s = table_ref[2 * far_rows + SIDE :, :]
        return far_c * near_c - far_s * near_s, far_s * near_c + far_c * near_s

    def rotate_keys(which):
        swap = swap_matrix(2 * HEAD_DIM)
        for block in which:
            cosine, sine = tables(block)
            raw = kve[block * SIDE : (block + 1) * SIDE, :]
            turned = jnp.dot(raw, swap, preferred_element_type=jnp.float32)
            krot[block * SIDE : (block + 1) * SIDE, :] = (
                raw.astype(jnp.float32) * cosine + turned * sine
            ).astype(jnp.bfloat16)

    heads = HEADS // KV_HEADS

    def attend(block):
        swap = swap_matrix(heads * HEAD_DIM)
        cosine, sine = tables(block + 1)
        cosine = jnp.concatenate([cosine] * (heads // 2), axis=1)
        sine = jnp.concatenate([sine] * (heads // 2), axis=1)
        raw = q_ref[block * SIDE : (block + 1) * SIDE, :]
        turned = jnp.dot(raw, swap, preferred_element_type=jnp.float32)
        query = (
            (raw.astype(jnp.float32) * cosine + turned * sine) * HEAD_DIM ** (-0.5)
        ).astype(jnp.bfloat16)
        query = jnp.concatenate(
            [query[:, h * HEAD_DIM : (h + 1) * HEAD_DIM] for h in range(heads)], axis=0
        )
        span = 3 * SIDE
        keys = krot[block * SIDE : block * SIDE + span, :HEAD_DIM]
        values = kve[block * SIDE : block * SIDE + span, HEAD_DIM:]
        scores = lax.dot_general(
            query, keys, (((1,), (1,)), ((), ())), preferred_element_type=jnp.float32
        )
        row = lax.broadcasted_iota(jnp.int32, scores.shape, 0) & (SIDE - 1)
        col = lax.broadcasted_iota(jnp.int32, scores.shape, 1)
        gap = col - row
        absolute = col + (ep * rows + (block - 1) * SIDE)
        allowed = (gap >= 0) & (gap <= 2 * HALF_WIN)
        allowed = allowed & (absolute >= 0) & (absolute < rows * 2 * chips)
        scores = jnp.where(allowed, scores, NEG_BIG)
        head = lax.broadcasted_iota(jnp.int32, (heads * SIDE, 1), 0) // SIDE
        sink = jnp.zeros((heads * SIDE, 1), jnp.float32)
        for h in range(heads):
            sink = jnp.where(head == h, sink_ref[h], sink)
        peak = jnp.maximum(jnp.max(scores, axis=1, keepdims=True), sink)
        lifted = jnp.exp(scores - peak)
        total = jnp.sum(lifted, axis=1, keepdims=True) + jnp.exp(sink - peak)
        out = jnp.dot(lifted.astype(jnp.bfloat16), values, preferred_element_type=jnp.float32)
        out = (out / total).astype(jnp.bfloat16)
        att[t, block * SIDE : (block + 1) * SIDE, :] = jnp.concatenate(
            [out[h * SIDE : (h + 1) * SIDE, :] for h in range(heads)], axis=1
        )

    def edges():
        arrive(("halo",), kve.at[pl.ds(0, 2 * SIDE)])
        rotate_keys((0, blocks + 1))

    tile = 256

    def gather(k):
        arrive(("p", k), own_rows(k, 1 - core))
        tag = xs[k, :, model:].astype(jnp.float32)
        lane = lax.broadcasted_iota(jnp.int32, tag.shape, 1)
        weight = jnp.sum(jnp.where(lane // 2 == core, tag, 0.0), axis=1, keepdims=True)
        wgt[...] = jnp.broadcast_to(weight, wgt.shape)

    def widen(k, start, stop):
        @pl.loop(start, stop)
        def _(i):
            at = pl.ds(pl.multiple_of(i * tile, tile), tile)
            gate = jnp.dot(xs[k, :, :model], wg[:, at], preferred_element_type=jnp.float32)
            lift = jnp.dot(xs[k, :, :model], wu[:, at], preferred_element_type=jnp.float32)
            value = gate / (1.0 + jnp.exp(-gate)) * lift
            weight = jnp.concatenate([wgt[...]] * (tile // wgt.shape[1]), axis=1)
            hid[:, at] = (value * weight).astype(jnp.bfloat16)

    last = chips - 1

    def target_of(i):
        return (t_d, t_y, t_x, t)[i]

    def narrow(k, i):
        target = target_of(i)
        at = pl.ds(pl.multiple_of(target * cols, cols), cols)
        yb[k, target] = jnp.dot(hid[...], wd[:, at], preferred_element_type=jnp.float32).astype(
            jnp.bfloat16
        )
        theirs = pl.ds(pl.multiple_of((1 - core) * cap, 16), cap)
        name = ("q", k, i) if k == last else ("q", k)
        send("q", name, yb.at[k, target, theirs], yr.at[k, target], (partner, t))

    def add(*parts):
        return sum(p.astype(jnp.float32) for p in parts).astype(jnp.bfloat16)

    first, second = slice(0, half_cap), slice(half_cap, cap)
    d_first, d_second = pl.ds(0, half_cap), pl.ds(half_cap, half_cap)

    def scatter_one(k, i):
        target = target_of(i)
        if k == last:
            arrive(("q", k, i), yr.at[k, target])
        elif i == 0:
            arrive(("q", k), yr.at[k])
        mine = pl.ds(pl.multiple_of(core * cap, 16), cap)
        zs[k, target] = add(yb[k, target, mine], yr[k, target])
        if i == 0:
            send("rx", ("rx", k), zs.at[k, t_d, d_first], rx.at[k, 1], (ep, t_x))
            send("ry", ("ry", k), zs.at[k, t_d, d_second], ry.at[k, 1], (ep, t_y))
        if i == 1:
            send("ry", ("g", k), zs.at[k, t_y, d_second], ry.at[k, 0], (ep, t_y))
        if i == 2:
            send("rx", ("g", k), zs.at[k, t_x, d_first], rx.at[k, 0], (ep, t_x))

    def scatter_two(k):
        arrive(("rx", k), rx.at[k, 1])
        sb[k, 0] = add(zs[k, t_y, first], rx[k, 1])
        send("r2", ("g", k), sb.at[k, 0], r2.at[k, 0], (ep, t_y))
        arrive(("ry", k), ry.at[k, 1])
        sb[k, 1] = add(zs[k, t_x, second], ry[k, 1])
        send("r2", ("g", k), sb.at[k, 1], r2.at[k, 1], (ep, t_x))

    def give_back(k):
        arrive(("g", k), r2.at[pl.ds(0, 2)])
        target = fin if k else ret
        target[k, first] = add(zs[k, t, first], rx[k, 0], r2[k, 0])
        target[k, second] = add(zs[k, t, second], ry[k, 0], r2[k, 1])
        if k:
            name = ("ret", last) if k == last else ("ret",)
            send("ret", name, fin.at[k], ret.at[k], (z_of[k] * 2 + core, t))

    def wait_back_early():
        arrive(("ret",), ret.at[pl.ds(1, last - 1)])

    def wait_back():
        arrive(("ret", last), ret.at[last])

    mid = pl.ds(SIDE, rows - 2 * SIDE)
    ends = (pl.ds(0, SIDE), pl.ds(rows - SIDE, SIDE))

    def attended_mid():
        send("ax", ("axm",), att.at[t, mid], att.at[t, mid], (ep, t_x))
        send("ay", ("proj",), att.at[t, mid], att.at[t, mid], (ep, t_y))

    def attended_ends():
        for at in ends:
            send("ay", ("aye",), att.at[t, at], att.at[t, at], (ep, t_y))
            send("ax", ("proj",), att.at[t, at], att.at[t, at], (ep, t_x))

    def attended_relay_mid():
        arrive(("axm",), att.at[t_x, mid])
        send("ad", ("proj",), att.at[t_x, mid], att.at[t_x, mid], (ep, t_y))

    def attended_relay_ends():
        arrive(("aye",), att.at[t_y, pl.ds(0, 2 * SIDE)])
        for at in ends:
            send("ad", ("proj",), att.at[t_y, at], att.at[t_y, at], (ep, t_x))

    def project():
        arrive(("proj",), att.at[pl.ds(0, 2)])
        width = att.shape[2]
        total = jnp.zeros((rows, cols), jnp.float32)
        for i in range(4):
            total += jnp.dot(
                att[i], wout[i * width : (i + 1) * width, :], preferred_element_type=jnp.float32
            )
        mixer_ref[...] = total.astype(jnp.bfloat16)

    def load_wait(i):
        loads[9 + i].wait()

    def place_early():
        count = (chips - 1) * cap
        acc[...] = jnp.dot(
            sel_ret[:, :count], ret[: chips - 1].reshape(count, cols),
            preferred_element_type=jnp.float32,
        )

    def place_last():
        count = (chips - 1) * cap
        expert_ref[...] = (
            acc[...]
            + jnp.dot(sel_ret[:, count:], ret[chips - 1], preferred_element_type=jnp.float32)
        ).astype(jnp.bfloat16)

    rotate_keys(range(1, blocks + 1))
    attend(1)
    attend(2)
    attended_mid()
    edges()
    attend(0)
    load_wait(0)
    load_wait(1)
    gather(0)
    widen(0, 0, 1)
    spread(1)
    widen(0, 1, 3)
    attended_relay_mid()
    attend(3)
    attended_ends()
    widen(0, 3, 4)
    share(1)
    load_wait(2)
    narrow(0, 0)
    narrow(0, 1)
    narrow(0, 2)
    narrow(0, 3)
    select_back()
    spread(2)
    gather(1)
    widen(1, 0, 1)
    scatter_one(0, 0)
    scatter_one(0, 1)
    scatter_one(0, 2)
    scatter_one(0, 3)
    widen(1, 1, 2)
    relay(2)
    spread(3)
    widen(1, 2, 4)
    attended_relay_ends()
    scatter_two(0)
    narrow(1, 0)
    narrow(1, 1)
    narrow(1, 2)
    narrow(1, 3)
    share(2)
    relay(3)
    scatter_one(1, 0)
    scatter_one(1, 1)
    scatter_one(1, 2)
    scatter_one(1, 3)
    gather(2)
    widen(2, 0, 2)
    share(3)
    give_back(0)
    widen(2, 2, 4)
    scatter_two(1)
    narrow(2, 0)
    narrow(2, 1)
    narrow(2, 2)
    narrow(2, 3)
    gather(3)
    widen(3, 0, 1)
    scatter_one(2, 0)
    scatter_one(2, 1)
    scatter_one(2, 2)
    scatter_one(2, 3)
    give_back(1)
    widen(3, 1, 4)
    scatter_two(2)
    narrow(3, 0)
    narrow(3, 1)
    narrow(3, 2)
    scatter_one(3, 0)
    narrow(3, 3)
    scatter_one(3, 1)
    scatter_one(3, 2)
    scatter_one(3, 3)
    give_back(2)
    load_wait(3)
    project()
    scatter_two(3)
    wait_back_early()
    place_early()
    give_back(3)
    wait_back()
    place_last()
    for family, ref in (
        ("halo", kve.at[pl.ds(0, 2 * SIDE)]), ("z", snd), ("p", xs.at[:, pl.ds(0, cap)]),
        ("x", snd.at[pl.ds(0, 3 * part)]), ("y", snd.at[pl.ds(0, 3 * part)]),
        ("d", snd.at[pl.ds(0, 2 * part)]), ("q", yr), ("rx", rx), ("ry", ry), ("r2", r2),
        ("ret", fin.at[pl.ds(1, last)]), ("ax", att.at[0]), ("ay", att.at[0]),
        ("ad", att.at[0]),
    ):
        sent(family, ref)


def local_fused(
    query_proj, key_proj, value_proj, sink_logit, out_weight, expert_input, norm_gain,
    routes, route_weights, gate_weight, up_weight, down_weight,
):
    rows = query_proj.shape[0]
    tokens, model = expert_input.shape
    cols = out_weight.shape[1]
    hidden = gate_weight.shape[2]
    cap = tokens // 2
    bf16, f32 = jnp.bfloat16, jnp.float32
    half = HEAD_DIM // 2
    channel = np.arange(2 * HEAD_DIM) % half
    inverse_freq = 1.0 / ROPE_BASE ** (channel * 2.0 / HEAD_DIM)
    far_count = -(-(lax.axis_size("ep") * (rows // SIDE) + 2) // 8) * 8
    far = (np.arange(far_count) - 1)[:, None] * SIDE * inverse_freq[None, :]
    near = np.arange(SIDE)[:, None] * inverse_freq[None, :]
    table = np.concatenate([np.cos(far), np.sin(far), np.cos(near), np.sin(near)]).astype(
        np.float32
    )
    hbm = pl.BlockSpec(memory_space=pltpu.HBM)
    vmem = pl.BlockSpec(memory_space=pltpu.VMEM)
    args = (
        expert_input, routes.T, route_weights.T, norm_gain[None, :], key_proj, value_proj,
        query_proj, jnp.asarray(table), sink_logit, gate_weight[0], up_weight[0], down_weight[0],
        out_weight,
    )
    scratch = [
        (pltpu.SMEM if a is sink_logit else pltpu.VMEM)(a.shape, a.dtype) for a in args
    ] + [
        pltpu.VMEM((rows + 2 * SIDE, 2 * HEAD_DIM), bf16),
        pltpu.VMEM((rows + 2 * SIDE, 2 * HEAD_DIM), bf16),
        pltpu.VMEM((4, rows, query_proj.shape[1]), bf16),
        pltpu.VMEM((tokens, GROUPS * cap), bf16),
        pltpu.VMEM((cap, model + 128), bf16),
        pltpu.VMEM((GROUPS, 2 * cap, model + 128), bf16),
        pltpu.VMEM((2 * cap, 128), f32),
        pltpu.VMEM((2 * cap, hidden), bf16),
        pltpu.VMEM((GROUPS, 4, 2 * cap, cols), bf16),
        pltpu.VMEM((GROUPS, 4, cap, cols), bf16),
        pltpu.VMEM((GROUPS, 4, cap, cols), bf16),
        pltpu.VMEM((GROUPS, 2, cap // 2, cols), bf16),
        pltpu.VMEM((GROUPS, 2, cap // 2, cols), bf16),
        pltpu.VMEM((GROUPS, 2, cap // 2, cols), bf16),
        pltpu.VMEM((GROUPS, 2, cap // 2, cols), bf16),
        pltpu.VMEM((GROUPS, cap, cols), bf16),
        pltpu.VMEM((GROUPS, cap, cols), bf16),
        pltpu.VMEM((tokens, cols), f32),
        pltpu.SemaphoreType.DMA((SEND_SLOTS,)),
        pltpu.SemaphoreType.DMA((RECV_SLOTS,)),
        pltpu.SemaphoreType.DMA((len(args) - 2,)),
    ]
    return pl.pallas_call(
        fused_kernel,
        out_shape=(pltpu.VMEM((rows, cols), bf16), pltpu.VMEM((tokens, cols), bf16)),
        in_specs=[hbm] * len(args),
        out_specs=(vmem, vmem),
        scratch_shapes=scratch,
        compiler_params=pltpu.CompilerParams(
            collective_id=0, has_side_effects=True, vmem_limit_bytes=60 * 1024 * 1024
        ),
    )(*args)


def solution(mesh):
    fused = fits_fused(mesh)
    return jax.shard_map(
        local_fused if fused else local,
        mesh=mesh,
        in_specs=(
            P("ep", "tp"),
            P("ep", None),
            P("ep", None),
            P("tp"),
            P(None, "tp"),
            P("ep", None),
            P(),
            P("ep", None),
            P("ep", None),
            P("ep", None, "tp"),
            P("ep", None, "tp"),
            P("ep", "tp", None),
        ),
        out_specs=(P("ep", "tp"), P("ep", "tp")),
        check_vma=False,
    )
```

```python
import jax
import jax.numpy as jnp
import numpy as np
from jax import lax
from jax.experimental import pallas as pl
from jax.experimental.pallas import tpu as pltpu
from jax.sharding import PartitionSpec as P

D = 2048
HEADS = 16
KV_HEADS = 4
HEAD_DIM = 64
HALF_WIN = 128
GROUPS = 4
TOP_K = 2


NORM_EPS = 1e-06
ROPE_BASE = 10000.0
NEG_BIG = -1e30
MESH = pl.DeviceIdType.MESH
SIDE = 128


def padded(block, sides, width):
    for axis, dim in sides:
        count = lax.axis_size(axis)
        forward = [(i, i + 1) for i in range(count - 1)]
        backward = [(target, source) for source, target in forward]
        low = lax.ppermute(
            lax.slice_in_dim(block, block.shape[dim] - width, None, axis=dim), axis, forward
        )
        high = lax.ppermute(lax.slice_in_dim(block, 0, width, axis=dim), axis, backward)
        block = jnp.concatenate([low, block, high], axis=dim)
    return block


def rotate(features, position_start):
    count = features.shape[0]
    half_dim = features.shape[-1] // 2
    inverse_freq = 1.0 / ROPE_BASE ** (
        jnp.arange(half_dim, dtype=jnp.float32) * 2.0 / features.shape[-1]
    )
    position = (jnp.arange(count, dtype=jnp.int32) + position_start).astype(jnp.float32)
    angles = position[:, None] * inverse_freq[None, :]
    cosine = jnp.cos(angles)[:, None, :]
    sine_part = jnp.sin(angles)[:, None, :]
    lower_half = features[..., :half_dim]
    upper_half = features[..., half_dim:]
    return jnp.concatenate(
        [
            lower_half * cosine - upper_half * sine_part,
            upper_half * cosine + lower_half * sine_part,
        ],
        axis=-1,
    )


def mixer_half(query_proj, key_proj, value_proj, sink_logit, out_weight):
    row_count = query_proj.shape[0]
    local_heads = query_proj.shape[1] // HEAD_DIM
    per_kv = HEADS // KV_HEADS
    kv_local = max(1, local_heads // per_kv)
    group_size = local_heads // kv_local
    tp_index = lax.axis_index("tp")
    offset = lax.axis_index("ep") * row_count
    seq_total = row_count * lax.axis_size("ep")
    first_kv = tp_index * local_heads // per_kv
    own_keys = lax.dynamic_slice_in_dim(key_proj, first_kv * HEAD_DIM, kv_local * HEAD_DIM, 1)
    own_values = lax.dynamic_slice_in_dim(value_proj, first_kv * HEAD_DIM, kv_local * HEAD_DIM, 1)
    rot_q = rotate(
        query_proj.reshape(row_count, local_heads, HEAD_DIM).astype(jnp.float32), offset
    ).astype(jnp.bfloat16)
    rot_k = rotate(
        own_keys.reshape(row_count, kv_local, HEAD_DIM).astype(jnp.float32), offset
    ).astype(jnp.bfloat16)
    stacked = jnp.stack([rot_k, own_values.reshape(row_count, kv_local, HEAD_DIM)])
    extended = padded(stacked, (("ep", 1),), HALF_WIN)
    own_sink = sink_logit.reshape(kv_local, group_size)
    block_rows = min(512, row_count)
    key_rows = block_rows + 2 * HALF_WIN
    key_offset = jnp.arange(key_rows, dtype=jnp.int32) - HALF_WIN
    key_gap = key_offset[None, :] - jnp.arange(block_rows, dtype=jnp.int32)[:, None]
    query_block = rot_q.reshape(block_rows, kv_local, group_size, HEAD_DIM)
    key_block = extended[0, 0:key_rows]
    value_block = extended[1, 0:key_rows]
    scores = jnp.einsum(
        "qngd,knd->ngqk", query_block, key_block, preferred_element_type=jnp.float32
    ) * HEAD_DIM ** (-0.5)
    global_key = offset + 0 + key_offset
    allowed = (
        (jnp.abs(key_gap) <= HALF_WIN)
        & (global_key >= 0)[None, :]
        & (global_key < seq_total)[None, :]
    )
    scores = jnp.where(allowed[None, None], scores, NEG_BIG)
    row_peak = jnp.maximum(jnp.max(scores, axis=-1), own_sink[:, :, None])
    lifted = jnp.exp(scores - row_peak[..., None])
    norm_total = jnp.sum(lifted, axis=-1) + jnp.exp(own_sink[:, :, None] - row_peak)
    probs = (lifted / norm_total[..., None]).astype(jnp.bfloat16)
    weighted = jnp.einsum("ngqk,knd->qngd", probs, value_block, preferred_element_type=jnp.float32)
    pieces = weighted.astype(jnp.bfloat16).reshape(block_rows, local_heads * HEAD_DIM)
    projected = jnp.dot(
        lax.all_gather(pieces, "tp", axis=1, tiled=True),
        out_weight,
        preferred_element_type=jnp.float32,
    )
    return projected.astype(jnp.bfloat16)


def expert_half(
    expert_input, norm_gain, routes, route_weights, gate_weight, up_weight, down_weight
):
    row_count = expert_input.shape[0]
    widened = expert_input.astype(jnp.float32)
    normed = (
        widened
        * lax.rsqrt(jnp.mean(widened * widened, axis=1, keepdims=True) + NORM_EPS)
        * norm_gain
    ).astype(jnp.bfloat16)
    local_experts = gate_weight.shape[0]
    ep_count = lax.axis_size("ep")
    expert_count = local_experts * ep_count
    capacity = row_count * GROUPS // expert_count
    col_count = D // lax.axis_size("tp")
    flat_routes = routes.reshape(-1)
    onehot = (flat_routes[:, None] == jnp.arange(expert_count, dtype=jnp.int32)[None, :]).astype(
        jnp.int32
    )
    slot_rank = jnp.sum((jnp.cumsum(onehot, axis=0) - onehot) * onehot, axis=1)
    slot_index = flat_routes * capacity + slot_rank
    source_rows = jnp.arange(row_count * TOP_K, dtype=jnp.int32) // TOP_K
    own_cols = lax.dynamic_slice_in_dim(normed, lax.axis_index("tp") * col_count, col_count, 1)
    outgoing = (
        jnp.zeros((expert_count * capacity, col_count), jnp.bfloat16)
        .at[slot_index]
        .set(own_cols[source_rows])
    )
    arrived = lax.all_to_all(
        outgoing.reshape(expert_count, capacity, col_count),
        "ep",
        split_axis=0,
        concat_axis=1,
        tiled=True,
    )
    shard_piece = lax.all_gather(arrived, "tp", axis=2, tiled=True)
    gate_sum = jnp.einsum(
        "esd,edh->esh", shard_piece, gate_weight, preferred_element_type=jnp.float32
    )
    up_sum = jnp.einsum("esd,edh->esh", shard_piece, up_weight, preferred_element_type=jnp.float32)
    hidden = (jax.nn.silu(gate_sum) * up_sum).astype(jnp.bfloat16)
    slot_total = hidden.shape[1]
    term = jnp.einsum("esh,ehc->ces", hidden, down_weight, preferred_element_type=jnp.float32)
    summed = lax.psum_scatter(
        term.reshape(col_count * lax.axis_size("tp"), local_experts * slot_total).astype(
            jnp.bfloat16
        ),
        "tp",
        scatter_dimension=0,
        tiled=True,
    )
    result = summed.reshape(col_count, local_experts, ep_count, capacity)
    returned = lax.all_to_all(result, "ep", split_axis=2, concat_axis=1, tiled=True)
    returned = returned.reshape(col_count, expert_count * capacity)
    picked = (
        jnp.take(returned, slot_index, axis=1)
        .reshape(col_count, row_count, TOP_K)
        .astype(jnp.float32)
    )
    combined = jnp.sum(picked * route_weights[None, :, :], axis=2)
    return combined.T.astype(jnp.bfloat16)


def local(
    query_proj,
    key_proj,
    value_proj,
    sink_logit,
    out_weight,
    expert_input,
    norm_gain,
    routes,
    route_weights,
    gate_weight,
    up_weight,
    down_weight,
):
    mixer_out = mixer_half(query_proj, key_proj, value_proj, sink_logit, out_weight)
    expert_out = expert_half(
        expert_input, norm_gain, routes, route_weights, gate_weight, up_weight, down_weight
    )
    return (mixer_out, expert_out)


def fits_fused(mesh):
    return (
        mesh.shape["tp"] == 4
        and mesh.shape["ep"] == 2 * GROUPS
        and HALF_WIN == SIDE
        and HEADS // KV_HEADS == 4
        and KV_HEADS == 4
    )


class Slots:
    def __init__(self):
        self.names = {}

    def __call__(self, *name):
        return self.names.setdefault(name, len(self.names))


RECV_SLOTS = 40
SEND_SLOTS = 14


def fused_kernel(
    x_hbm, routes_hbm, rw_hbm, gain_hbm, key_hbm, value_hbm, q_hbm, table_hbm, sink_hbm,
    wg_hbm, wu_hbm, wd_hbm, wout_hbm,
    mixer_ref, expert_ref,
    x_ref, routes_ref, rw_ref, gain_ref, key_ref, value_ref, q_ref, table_ref, sink_ref,
    wg, wu, wd, wout,
    kve, krot, att, sel_ret, snd, xs, wgt, hid, yb, yr, zs, rx, ry, sb, r2, fin, ret, acc,
    ssem, rsem, wsem,
):
    ep = lax.axis_index("ep")
    t = lax.axis_index("tp")
    chips = GROUPS
    z, core = ep // 2, ep % 2
    partner = ep + 1 - 2 * core
    other = (ep + 2 * core - 1 + 2 * chips) % (2 * chips)
    up, down = (ep + 1) % (2 * chips), (ep + 2 * chips - 1) % (2 * chips)
    ty, tx = t // 2, t % 2
    t_x, t_y, t_d = ty * 2 + 1 - tx, (1 - ty) * 2 + tx, (1 - ty) * 2 + 1 - tx
    rows = q_ref.shape[0]
    tokens, model = x_ref.shape
    cap = xs.shape[1] // 2
    part = cap // 4
    half_part, half_cap = part // 2, cap // 2
    hidden = wg.shape[1]
    cols = wout.shape[1]
    slots, send_slots = Slots(), Slots()
    z_of = (z, z + 1 - 2 * (z % 2), (z + 2) % chips, chips - 1 - z)

    def remote(send_index, recv_index, src, dst, device):
        return pltpu.make_async_remote_copy(
            src_ref=src, dst_ref=dst, send_sem=ssem.at[send_index], recv_sem=rsem.at[recv_index],
            device_id=device, device_id_type=MESH,
        )

    def send(family, name, src, dst, device):
        remote(send_slots(family), slots(*name), src, dst, device).start()

    def arrive(name, dst):
        remote(0, slots(*name), dst, dst, (ep, t_x)).wait_recv()

    def sent(family, src):
        remote(send_slots(family), 0, src, src, (ep, t_x)).wait_send()

    barrier = pltpu.get_barrier_semaphore()
    peers = [(z_of[k] * 2 + core, t) for k in range(1, chips)]
    peers += [(ep, t_x), (ep, t_y), (partner, t), (other, t)]
    for peer in peers:
        pl.semaphore_signal(barrier, inc=1, device_id=peer, device_id_type=MESH)

    pairs = (
        (x_hbm, x_ref), (routes_hbm, routes_ref), (rw_hbm, rw_ref), (gain_hbm, gain_ref),
        (key_hbm, key_ref), (value_hbm, value_ref), (q_hbm, q_ref), (table_hbm, table_ref),
        (sink_hbm, sink_ref), (wg_hbm, wg), (wu_hbm, wu), (wd_hbm, wd), (wout_hbm, wout),
    )
    order = (0, 1, 2, 3, 4, 4, 4, 5, 6, 7, 8, 9, 10)
    loads = [pltpu.make_async_copy(a, b, wsem.at[i]) for i, (a, b) in zip(order, pairs)]
    for copy in loads[:9]:
        copy.start()
    for copy in loads[:4]:
        copy.wait()
    for copy in loads[9:]:
        copy.start()

    wide = x_ref[...].astype(jnp.float32)
    inverse = lax.rsqrt(jnp.mean(wide * wide, axis=1, keepdims=True) + NORM_EPS)
    normed = (wide * inverse * gain_ref[...]).astype(jnp.bfloat16)
    group = routes_ref[0:1, :] >> 1
    row_i = lax.broadcasted_iota(jnp.int32, (tokens, tokens), 0)
    col_i = lax.broadcasted_iota(jnp.int32, (tokens, tokens), 1)
    later = jnp.where(row_i < col_i, 1.0, 0.0).astype(jnp.bfloat16)
    hot = jnp.where(lax.broadcasted_iota(jnp.int32, (16, tokens), 0) == group, 1.0, 0.0)
    count = jnp.dot(hot.astype(jnp.bfloat16), later, preferred_element_type=jnp.float32)
    rank = jnp.sum(count * hot, axis=0, keepdims=True).astype(jnp.int32)

    odd = (routes_ref[...] & 1) == 1
    weight_odd = jnp.sum(jnp.where(odd, rw_ref[...], 0.0), axis=0, keepdims=True)
    weight_even = jnp.sum(jnp.where(odd, 0.0, rw_ref[...]), axis=0, keepdims=True)
    lane = lax.broadcasted_iota(jnp.int32, (128, tokens), 0)
    weight = jnp.where(lane < 2, weight_even, weight_odd)
    high = weight.astype(jnp.bfloat16).astype(jnp.float32)
    weight = jnp.where((lane & 1) == 0, high, weight - high)
    weight = jnp.where(lane < 4, weight, 0.0).astype(jnp.bfloat16)

    def select(pick, out, at):
        pick = jnp.where(pick, 1.0, 0.0).astype(jnp.bfloat16)
        out[at, model:] = lax.dot_general(
            pick, weight, (((1,), (1,)), ((), ())), preferred_element_type=jnp.float32
        ).astype(jnp.bfloat16)
        out[at, :model] = jnp.dot(pick, normed, preferred_element_type=jnp.float32).astype(
            jnp.bfloat16
        )

    def group_at(index):
        return jnp.where(
            index == 0, z_of[0],
            jnp.where(index == 1, z_of[1], jnp.where(index == 2, z_of[2], z_of[3])),
        )

    pieces = ((1, t, "z"), (2, t, "z"), (1, t_d, "s"), (3, t, "z"), (3, t_d, "s"))
    slot = lax.broadcasted_iota(jnp.int32, (len(pieces) * part, tokens), 0)
    index = slot // part
    owner = jnp.where((index == 2) | (index == 4), t_d, t)
    step = jnp.where(index == 1, 2, jnp.where(index >= 3, 3, 1))
    select(
        (group == group_at(step)) & (rank == owner * part + lax.rem(slot, part)), snd,
        slice(0, len(pieces) * part),
    )

    def piece(k, owner_t, start=0, count=part):
        first = pl.multiple_of(core * cap + owner_t * part + start, 16)
        return xs.at[k, pl.ds(first, count)]

    def own_rows(k, which):
        return xs.at[k, pl.ds(pl.multiple_of(which * cap, 16), cap)]

    pltpu.make_async_copy(att.at[pl.ds(0, 3)], att.at[pl.ds(0, 3)], wsem.at[4]).wait()
    for copy in loads[7:9]:
        copy.wait()
    row_i = lax.broadcasted_iota(jnp.int32, (key_ref.shape[1], 2 * HEAD_DIM), 0)
    col_i = lax.broadcasted_iota(jnp.int32, (key_ref.shape[1], 2 * HEAD_DIM), 1)
    own_key = jnp.where((row_i == t * HEAD_DIM + col_i) & (col_i < HEAD_DIM), 1.0, 0.0)
    own_value = jnp.where(
        (row_i == (t - 1) * HEAD_DIM + col_i) & (col_i >= HEAD_DIM), 1.0, 0.0
    )
    both = jnp.dot(
        key_ref[...], own_key.astype(jnp.bfloat16), preferred_element_type=jnp.float32
    ) + jnp.dot(
        value_ref[...], own_value.astype(jnp.bfloat16), preferred_element_type=jnp.float32
    )
    kve[SIDE : SIDE + rows, :] = both.astype(jnp.bfloat16)

    pl.semaphore_wait(barrier, len(peers))
    send("halo", ("halo",), kve.at[pl.ds(rows, SIDE)], kve.at[pl.ds(0, SIDE)], (up, t))
    send("halo", ("halo",), kve.at[pl.ds(SIDE, SIDE)], kve.at[pl.ds(SIDE + rows, SIDE)], (down, t))
    def dispatch(i):
        k, owner_t, name = pieces[i]
        send(
            "z", (name, k), snd.at[pl.ds(i * part, part)], piece(k, owner_t),
            (z_of[k] * 2 + core, t),
        )

    dispatch(0)

    slot = lax.broadcasted_iota(jnp.int32, (cap, tokens), 0)
    select(
        (group == z) & (rank == slot), xs.at[0], pl.ds(pl.multiple_of(core * cap, 16), cap)
    )
    send("p", ("p", 0), own_rows(0, core), own_rows(0, core), (partner, t))

    def select_back():
        slot = lax.broadcasted_iota(jnp.int32, (chips * cap, tokens), 0)
        place = (group == group_at(slot // cap)) & (rank == lax.rem(slot, cap))
        sel_ret[...] = jnp.where(place, 1.0, 0.0).T.astype(jnp.bfloat16)

    def spread(k):
        arrive(("z", k), piece(k, t))
        if k != 2:
            send("x", ("s", k), piece(k, t), piece(k, t), (ep, t_x))
            send("y", ("s", k), piece(k, t), piece(k, t), (ep, t_y))
            return
        for family, name, start, device in (
            ("x", "xl", 0, t_x), ("y", "yh", half_part, t_y),
            ("x", "s", half_part, t_x), ("y", "s", 0, t_y),
        ):
            rows_of = piece(k, t, start, half_part)
            send(family, (name, k), rows_of, rows_of, (ep, device))

    def relay(k, half):
        name, source, target = (("xl", t_x, t_y), ("yh", t_y, t_x))[half]
        rows_of = piece(k, source, half * half_part, half_part)
        arrive((name, k), rows_of)
        send("d", ("s", k), rows_of, rows_of, (ep, target))

    def share(k):
        arrive(("s", k), snd.at[pl.ds(0, (2 if k == 2 else 3) * part)])
        send("p", ("p", k), own_rows(k, core), own_rows(k, core), (partner, t))

    def swap_matrix(size):
        i = lax.broadcasted_iota(jnp.int32, (size, size), 0)
        j = lax.broadcasted_iota(jnp.int32, (size, size), 1)
        half = HEAD_DIM // 2
        low = (j & (HEAD_DIM - 1)) < half
        minus = low & (i == j + half)
        plus = (~low) & (i == j - half)
        return jnp.where(minus, -1.0, jnp.where(plus, 1.0, 0.0)).astype(jnp.bfloat16)

    blocks = rows // SIDE
    far_rows = (table_ref.shape[0] - 2 * SIDE) // 2

    def tables(block):
        at = ep * blocks + block
        far_c = table_ref[pl.ds(at, 1), :]
        far_s = table_ref[pl.ds(far_rows + at, 1), :]
        near_c = table_ref[2 * far_rows : 2 * far_rows + SIDE, :]
        near_s = table_ref[2 * far_rows + SIDE :, :]
        return far_c * near_c - far_s * near_s, far_s * near_c + far_c * near_s

    def rotate_keys(which):
        swap = swap_matrix(2 * HEAD_DIM)
        for block in which:
            cosine, sine = tables(block)
            raw = kve[block * SIDE : (block + 1) * SIDE, :]
            turned = jnp.dot(raw, swap, preferred_element_type=jnp.float32)
            krot[block * SIDE : (block + 1) * SIDE, :] = (
                raw.astype(jnp.float32) * cosine + turned * sine
            ).astype(jnp.bfloat16)

    heads = HEADS // KV_HEADS

    def attend(block):
        swap = swap_matrix(heads * HEAD_DIM)
        cosine, sine = tables(block + 1)
        cosine = jnp.concatenate([cosine] * (heads // 2), axis=1)
        sine = jnp.concatenate([sine] * (heads // 2), axis=1)
        raw = q_ref[block * SIDE : (block + 1) * SIDE, :]
        turned = jnp.dot(raw, swap, preferred_element_type=jnp.float32)
        query = (
            (raw.astype(jnp.float32) * cosine + turned * sine) * HEAD_DIM ** (-0.5)
        ).astype(jnp.bfloat16)
        query = jnp.concatenate(
            [query[:, h * HEAD_DIM : (h + 1) * HEAD_DIM] for h in range(heads)], axis=0
        )
        span = 3 * SIDE
        keys = krot[block * SIDE : block * SIDE + span, :HEAD_DIM]
        values = kve[block * SIDE : block * SIDE + span, HEAD_DIM:]
        scores = lax.dot_general(
            query, keys, (((1,), (1,)), ((), ())), preferred_element_type=jnp.float32
        )
        row = lax.broadcasted_iota(jnp.int32, scores.shape, 0) & (SIDE - 1)
        col = lax.broadcasted_iota(jnp.int32, scores.shape, 1)
        gap = col - row
        absolute = col + (ep * rows + (block - 1) * SIDE)
        allowed = (gap >= 0) & (gap <= 2 * HALF_WIN)
        allowed = allowed & (absolute >= 0) & (absolute < rows * 2 * chips)
        scores = jnp.where(allowed, scores, NEG_BIG)
        head = lax.broadcasted_iota(jnp.int32, (heads * SIDE, 1), 0) // SIDE
        sink = jnp.zeros((heads * SIDE, 1), jnp.float32)
        for h in range(heads):
            sink = jnp.where(head == h, sink_ref[h], sink)
        peak = jnp.maximum(jnp.max(scores, axis=1, keepdims=True), sink)
        lifted = jnp.exp(scores - peak)
        total = jnp.sum(lifted, axis=1, keepdims=True) + jnp.exp(sink - peak)
        out = jnp.dot(lifted.astype(jnp.bfloat16), values, preferred_element_type=jnp.float32)
        out = (out / total).astype(jnp.bfloat16)
        att[t, block * SIDE : (block + 1) * SIDE, :] = jnp.concatenate(
            [out[h * SIDE : (h + 1) * SIDE, :] for h in range(heads)], axis=1
        )

    def edges():
        arrive(("halo",), kve.at[pl.ds(0, 2 * SIDE)])
        rotate_keys((0, blocks + 1))

    tile = 256

    def gather(k):
        arrive(("p", k), own_rows(k, 1 - core))
        tag = xs[k, :, model:].astype(jnp.float32)
        lane = lax.broadcasted_iota(jnp.int32, tag.shape, 1)
        weight = jnp.sum(jnp.where(lane // 2 == core, tag, 0.0), axis=1, keepdims=True)
        wgt[...] = jnp.broadcast_to(weight, wgt.shape)

    def widen(k, start, stop):
        for i in range(start, stop):
            at = pl.ds(i * tile, tile)
            gate = jnp.dot(xs[k, :, :model], wg[:, at], preferred_element_type=jnp.float32)
            lift = jnp.dot(xs[k, :, :model], wu[:, at], preferred_element_type=jnp.float32)
            value = gate / (1.0 + jnp.exp(-gate)) * lift
            weight = jnp.concatenate([wgt[...]] * (tile // wgt.shape[1]), axis=1)
            hid[:, at] = (value * weight).astype(jnp.bfloat16)

    last = chips - 1

    def target_of(i):
        return (t_d, t_y, t_x, t)[i]

    def narrow(k, i):
        target = target_of(i)
        at = pl.ds(pl.multiple_of(target * cols, cols), cols)
        yb[k, target] = jnp.dot(hid[...], wd[:, at], preferred_element_type=jnp.float32).astype(
            jnp.bfloat16
        )
        theirs = pl.ds(pl.multiple_of((1 - core) * cap, 16), cap)
        name = ("q", k, i) if k >= 2 else ("q", k)
        send("q", name, yb.at[k, target, theirs], yr.at[k, target], (partner, t))

    def add(*parts):
        return sum(p.astype(jnp.float32) for p in parts).astype(jnp.bfloat16)

    first, second = slice(0, half_cap), slice(half_cap, cap)
    d_first, d_second = pl.ds(0, half_cap), pl.ds(half_cap, half_cap)

    def scatter_add(k, i):
        target = target_of(i)
        if k >= 2:
            arrive(("q", k, i), yr.at[k, target])
        elif i == 0:
            arrive(("q", k), yr.at[k])
        mine = pl.ds(pl.multiple_of(core * cap, 16), cap)
        zs[k, target] = add(yb[k, target, mine], yr[k, target])

    def scatter_send(k, i):
        if i == 0:
            send("rx", ("rx", k), zs.at[k, t_d, d_first], rx.at[k, 1], (ep, t_x))
            send("ry", ("ry", k), zs.at[k, t_d, d_second], ry.at[k, 1], (ep, t_y))
        if i == 1:
            send("ry", ("g", k), zs.at[k, t_y, d_second], ry.at[k, 0], (ep, t_y))
        if i == 2:
            send("rx", ("g", k), zs.at[k, t_x, d_first], rx.at[k, 0], (ep, t_x))

    def scatter_one(k, i):
        scatter_add(k, i)
        scatter_send(k, i)

    def scatter_two(k):
        arrive(("rx", k), rx.at[k, 1])
        sb[k, 0] = add(zs[k, t_y, first], rx[k, 1])
        send("r2", ("g", k), sb.at[k, 0], r2.at[k, 0], (ep, t_y))
        arrive(("ry", k), ry.at[k, 1])
        sb[k, 1] = add(zs[k, t_x, second], ry[k, 1])
        send("r2", ("g", k), sb.at[k, 1], r2.at[k, 1], (ep, t_x))

    def give_back(k):
        arrive(("g", k), r2.at[pl.ds(0, 2)])
        target = fin if k else ret
        target[k, first] = add(zs[k, t, first], rx[k, 0], r2[k, 0])
        target[k, second] = add(zs[k, t, second], ry[k, 0], r2[k, 1])
        if k:
            name = ("ret", last) if k == last else ("ret",)
            send("ret", name, fin.at[k], ret.at[k], (z_of[k] * 2 + core, t))

    def wait_back_early():
        arrive(("ret",), ret.at[pl.ds(1, last - 1)])

    def wait_back():
        arrive(("ret", last), ret.at[last])

    mid = pl.ds(SIDE, rows - 2 * SIDE)
    ends = (pl.ds(0, SIDE), pl.ds(rows - SIDE, SIDE))

    def attended_mid():
        send("ax", ("axm",), att.at[t, mid], att.at[t, mid], (ep, t_x))
        send("ay", ("proj",), att.at[t, mid], att.at[t, mid], (ep, t_y))

    def attended_ends():
        for at in ends:
            send("ay", ("aye",), att.at[t, at], att.at[t, at], (ep, t_y))
            send("ax", ("proj",), att.at[t, at], att.at[t, at], (ep, t_x))

    def attended_relay_mid():
        arrive(("axm",), att.at[t_x, mid])
        send("ad", ("proj",), att.at[t_x, mid], att.at[t_x, mid], (ep, t_y))

    def attended_relay_ends():
        arrive(("aye",), att.at[t_y, pl.ds(0, 2 * SIDE)])
        for at in ends:
            send("ad", ("proj",), att.at[t_y, at], att.at[t_y, at], (ep, t_x))

    def project():
        arrive(("proj",), att.at[pl.ds(0, 2)])
        width = att.shape[2]
        total = jnp.zeros((rows, cols), jnp.float32)
        for i in range(4):
            total += jnp.dot(
                att[i], wout[i * width : (i + 1) * width, :], preferred_element_type=jnp.float32
            )
        mixer_ref[...] = total.astype(jnp.bfloat16)

    def load_wait(i):
        loads[9 + i].wait()

    def place_early():
        count = (chips - 1) * cap
        acc[...] = jnp.dot(
            sel_ret[:, :count], ret[: chips - 1].reshape(count, cols),
            preferred_element_type=jnp.float32,
        )

    def place_last():
        count = (chips - 1) * cap
        expert_ref[...] = (
            acc[...]
            + jnp.dot(sel_ret[:, count:], ret[chips - 1], preferred_element_type=jnp.float32)
        ).astype(jnp.bfloat16)

    rotate_keys(range(1, blocks + 1))
    attend(1)
    dispatch(1)
    dispatch(2)
    attend(2)
    attended_mid()
    dispatch(3)
    edges()
    attend(0)
    attend(3)
    attended_ends()
    load_wait(0)
    load_wait(1)
    gather(0)
    widen(0, 0, 2)
    spread(1)
    widen(0, 2, 4)
    load_wait(2)
    narrow(0, 0)
    narrow(0, 1)
    narrow(0, 2)
    narrow(0, 3)
    spread(2)
    dispatch(4)
    select_back()
    share(1)
    relay(2, 0)
    scatter_add(0, 0)
    scatter_add(0, 1)
    scatter_add(0, 2)
    scatter_add(0, 3)
    gather(1)
    relay(2, 1)
    widen(1, 0, 2)
    attended_relay_mid()
    attended_relay_ends()
    widen(1, 2, 4)
    narrow(1, 0)
    spread(3)
    narrow(1, 1)
    narrow(1, 2)
    share(2)
    narrow(1, 3)
    scatter_send(0, 0)
    scatter_send(0, 1)
    scatter_send(0, 2)
    gather(2)
    widen(2, 0, 1)
    scatter_one(1, 0)
    scatter_one(1, 1)
    scatter_one(1, 2)
    scatter_one(1, 3)
    widen(2, 1, 4)
    narrow(2, 0)
    narrow(2, 1)
    share(3)
    scatter_one(2, 0)
    narrow(2, 2)
    scatter_one(2, 1)
    narrow(2, 3)
    scatter_one(2, 2)
    gather(3)
    widen(3, 0, 1)
    scatter_one(2, 3)
    scatter_two(1)
    widen(3, 1, 4)
    narrow(3, 0)
    narrow(3, 1)
    scatter_two(2)
    narrow(3, 2)
    scatter_one(3, 0)
    narrow(3, 3)
    scatter_one(3, 1)
    scatter_one(3, 2)
    scatter_one(3, 3)
    give_back(1)
    load_wait(3)
    project()
    give_back(2)
    scatter_two(3)
    scatter_two(0)
    give_back(3)
    give_back(0)
    wait_back_early()
    place_early()
    wait_back()
    place_last()
    for family, ref in (
        ("halo", kve.at[pl.ds(0, 2 * SIDE)]), ("z", snd), ("p", xs.at[:, pl.ds(0, cap)]),
        ("x", snd.at[pl.ds(0, 3 * part)]), ("y", snd.at[pl.ds(0, 3 * part)]),
        ("d", snd.at[pl.ds(0, part)]), ("q", yr), ("rx", rx), ("ry", ry), ("r2", r2),
        ("ret", fin.at[pl.ds(1, last)]), ("ax", att.at[0]), ("ay", att.at[0]),
        ("ad", att.at[0]),
    ):
        sent(family, ref)


def local_fused(
    query_proj, key_proj, value_proj, sink_logit, out_weight, expert_input, norm_gain,
    routes, route_weights, gate_weight, up_weight, down_weight,
):
    rows = query_proj.shape[0]
    tokens, model = expert_input.shape
    cols = out_weight.shape[1]
    hidden = gate_weight.shape[2]
    cap = tokens // 2
    bf16, f32 = jnp.bfloat16, jnp.float32
    half = HEAD_DIM // 2
    channel = np.arange(2 * HEAD_DIM) % half
    inverse_freq = 1.0 / ROPE_BASE ** (channel * 2.0 / HEAD_DIM)
    far_count = -(-(lax.axis_size("ep") * (rows // SIDE) + 2) // 8) * 8
    far = (np.arange(far_count) - 1)[:, None] * SIDE * inverse_freq[None, :]
    near = np.arange(SIDE)[:, None] * inverse_freq[None, :]
    table = np.concatenate([np.cos(far), np.sin(far), np.cos(near), np.sin(near)]).astype(
        np.float32
    )
    hbm = pl.BlockSpec(memory_space=pltpu.HBM)
    vmem = pl.BlockSpec(memory_space=pltpu.VMEM)
    args = (
        expert_input, routes.T, route_weights.T, norm_gain[None, :], key_proj, value_proj,
        query_proj, jnp.asarray(table), sink_logit, gate_weight[0], up_weight[0], down_weight[0],
        out_weight,
    )
    scratch = [
        (pltpu.SMEM if a is sink_logit else pltpu.VMEM)(a.shape, a.dtype) for a in args
    ] + [
        pltpu.VMEM((rows + 2 * SIDE, 2 * HEAD_DIM), bf16),
        pltpu.VMEM((rows + 2 * SIDE, 2 * HEAD_DIM), bf16),
        pltpu.VMEM((4, rows, query_proj.shape[1]), bf16),
        pltpu.VMEM((tokens, GROUPS * cap), bf16),
        pltpu.VMEM((5 * cap // 4, model + 128), bf16),
        pltpu.VMEM((GROUPS, 2 * cap, model + 128), bf16),
        pltpu.VMEM((2 * cap, 128), f32),
        pltpu.VMEM((2 * cap, hidden), bf16),
        pltpu.VMEM((GROUPS, 4, 2 * cap, cols), bf16),
        pltpu.VMEM((GROUPS, 4, cap, cols), bf16),
        pltpu.VMEM((GROUPS, 4, cap, cols), bf16),
        pltpu.VMEM((GROUPS, 2, cap // 2, cols), bf16),
        pltpu.VMEM((GROUPS, 2, cap // 2, cols), bf16),
        pltpu.VMEM((GROUPS, 2, cap // 2, cols), bf16),
        pltpu.VMEM((GROUPS, 2, cap // 2, cols), bf16),
        pltpu.VMEM((GROUPS, cap, cols), bf16),
        pltpu.VMEM((GROUPS, cap, cols), bf16),
        pltpu.VMEM((tokens, cols), f32),
        pltpu.SemaphoreType.DMA((SEND_SLOTS,)),
        pltpu.SemaphoreType.DMA((RECV_SLOTS,)),
        pltpu.SemaphoreType.DMA((len(args) - 2,)),
    ]
    return pl.pallas_call(
        fused_kernel,
        out_shape=(pltpu.VMEM((rows, cols), bf16), pltpu.VMEM((tokens, cols), bf16)),
        in_specs=[hbm] * len(args),
        out_specs=(vmem, vmem),
        scratch_shapes=scratch,
        compiler_params=pltpu.CompilerParams(
            collective_id=0, has_side_effects=True, vmem_limit_bytes=60 * 1024 * 1024
        ),
    )(*args)


def solution(mesh):
    fused = fits_fused(mesh)
    return jax.shard_map(
        local_fused if fused else local,
        mesh=mesh,
        in_specs=(
            P("ep", "tp"),
            P("ep", None),
            P("ep", None),
            P("tp"),
            P(None, "tp"),
            P("ep", None),
            P(),
            P("ep", None),
            P("ep", None),
            P("ep", None, "tp"),
            P("ep", None, "tp"),
            P("ep", "tp", None),
        ),
        out_specs=(P("ep", "tp"), P("ep", "tp")),
        check_vma=False,
    )
```

```python
import jax
import jax.numpy as jnp
import numpy as np
from jax import lax
from jax.experimental import pallas as pl
from jax.experimental.pallas import tpu as pltpu
from jax.sharding import PartitionSpec as P

D = 2048
HEADS = 16
KV_HEADS = 4
HEAD_DIM = 64
HALF_WIN = 128
GROUPS = 4
TOP_K = 2


NORM_EPS = 1e-06
ROPE_BASE = 10000.0
NEG_BIG = -1e30
MESH = pl.DeviceIdType.MESH
SIDE = 128


def padded(block, sides, width):
    for axis, dim in sides:
        count = lax.axis_size(axis)
        forward = [(i, i + 1) for i in range(count - 1)]
        backward = [(target, source) for source, target in forward]
        low = lax.ppermute(
            lax.slice_in_dim(block, block.shape[dim] - width, None, axis=dim), axis, forward
        )
        high = lax.ppermute(lax.slice_in_dim(block, 0, width, axis=dim), axis, backward)
        block = jnp.concatenate([low, block, high], axis=dim)
    return block


def rotate(features, position_start):
    count = features.shape[0]
    half_dim = features.shape[-1] // 2
    inverse_freq = 1.0 / ROPE_BASE ** (
        jnp.arange(half_dim, dtype=jnp.float32) * 2.0 / features.shape[-1]
    )
    position = (jnp.arange(count, dtype=jnp.int32) + position_start).astype(jnp.float32)
    angles = position[:, None] * inverse_freq[None, :]
    cosine = jnp.cos(angles)[:, None, :]
    sine_part = jnp.sin(angles)[:, None, :]
    lower_half = features[..., :half_dim]
    upper_half = features[..., half_dim:]
    return jnp.concatenate(
        [
            lower_half * cosine - upper_half * sine_part,
            upper_half * cosine + lower_half * sine_part,
        ],
        axis=-1,
    )


def mixer_half(query_proj, key_proj, value_proj, sink_logit, out_weight):
    row_count = query_proj.shape[0]
    local_heads = query_proj.shape[1] // HEAD_DIM
    per_kv = HEADS // KV_HEADS
    kv_local = max(1, local_heads // per_kv)
    group_size = local_heads // kv_local
    tp_index = lax.axis_index("tp")
    offset = lax.axis_index("ep") * row_count
    seq_total = row_count * lax.axis_size("ep")
    first_kv = tp_index * local_heads // per_kv
    own_keys = lax.dynamic_slice_in_dim(key_proj, first_kv * HEAD_DIM, kv_local * HEAD_DIM, 1)
    own_values = lax.dynamic_slice_in_dim(value_proj, first_kv * HEAD_DIM, kv_local * HEAD_DIM, 1)
    rot_q = rotate(
        query_proj.reshape(row_count, local_heads, HEAD_DIM).astype(jnp.float32), offset
    ).astype(jnp.bfloat16)
    rot_k = rotate(
        own_keys.reshape(row_count, kv_local, HEAD_DIM).astype(jnp.float32), offset
    ).astype(jnp.bfloat16)
    stacked = jnp.stack([rot_k, own_values.reshape(row_count, kv_local, HEAD_DIM)])
    extended = padded(stacked, (("ep", 1),), HALF_WIN)
    own_sink = sink_logit.reshape(kv_local, group_size)
    block_rows = min(512, row_count)
    key_rows = block_rows + 2 * HALF_WIN
    key_offset = jnp.arange(key_rows, dtype=jnp.int32) - HALF_WIN
    key_gap = key_offset[None, :] - jnp.arange(block_rows, dtype=jnp.int32)[:, None]
    query_block = rot_q.reshape(block_rows, kv_local, group_size, HEAD_DIM)
    key_block = extended[0, 0:key_rows]
    value_block = extended[1, 0:key_rows]
    scores = jnp.einsum(
        "qngd,knd->ngqk", query_block, key_block, preferred_element_type=jnp.float32
    ) * HEAD_DIM ** (-0.5)
    global_key = offset + 0 + key_offset
    allowed = (
        (jnp.abs(key_gap) <= HALF_WIN)
        & (global_key >= 0)[None, :]
        & (global_key < seq_total)[None, :]
    )
    scores = jnp.where(allowed[None, None], scores, NEG_BIG)
    row_peak = jnp.maximum(jnp.max(scores, axis=-1), own_sink[:, :, None])
    lifted = jnp.exp(scores - row_peak[..., None])
    norm_total = jnp.sum(lifted, axis=-1) + jnp.exp(own_sink[:, :, None] - row_peak)
    probs = (lifted / norm_total[..., None]).astype(jnp.bfloat16)
    weighted = jnp.einsum("ngqk,knd->qngd", probs, value_block, preferred_element_type=jnp.float32)
    pieces = weighted.astype(jnp.bfloat16).reshape(block_rows, local_heads * HEAD_DIM)
    projected = jnp.dot(
        lax.all_gather(pieces, "tp", axis=1, tiled=True),
        out_weight,
        preferred_element_type=jnp.float32,
    )
    return projected.astype(jnp.bfloat16)


def expert_half(
    expert_input, norm_gain, routes, route_weights, gate_weight, up_weight, down_weight
):
    row_count = expert_input.shape[0]
    widened = expert_input.astype(jnp.float32)
    normed = (
        widened
        * lax.rsqrt(jnp.mean(widened * widened, axis=1, keepdims=True) + NORM_EPS)
        * norm_gain
    ).astype(jnp.bfloat16)
    local_experts = gate_weight.shape[0]
    ep_count = lax.axis_size("ep")
    expert_count = local_experts * ep_count
    capacity = row_count * GROUPS // expert_count
    col_count = D // lax.axis_size("tp")
    flat_routes = routes.reshape(-1)
    onehot = (flat_routes[:, None] == jnp.arange(expert_count, dtype=jnp.int32)[None, :]).astype(
        jnp.int32
    )
    slot_rank = jnp.sum((jnp.cumsum(onehot, axis=0) - onehot) * onehot, axis=1)
    slot_index = flat_routes * capacity + slot_rank
    source_rows = jnp.arange(row_count * TOP_K, dtype=jnp.int32) // TOP_K
    own_cols = lax.dynamic_slice_in_dim(normed, lax.axis_index("tp") * col_count, col_count, 1)
    outgoing = (
        jnp.zeros((expert_count * capacity, col_count), jnp.bfloat16)
        .at[slot_index]
        .set(own_cols[source_rows])
    )
    arrived = lax.all_to_all(
        outgoing.reshape(expert_count, capacity, col_count),
        "ep",
        split_axis=0,
        concat_axis=1,
        tiled=True,
    )
    shard_piece = lax.all_gather(arrived, "tp", axis=2, tiled=True)
    gate_sum = jnp.einsum(
        "esd,edh->esh", shard_piece, gate_weight, preferred_element_type=jnp.float32
    )
    up_sum = jnp.einsum("esd,edh->esh", shard_piece, up_weight, preferred_element_type=jnp.float32)
    hidden = (jax.nn.silu(gate_sum) * up_sum).astype(jnp.bfloat16)
    slot_total = hidden.shape[1]
    term = jnp.einsum("esh,ehc->ces", hidden, down_weight, preferred_element_type=jnp.float32)
    summed = lax.psum_scatter(
        term.reshape(col_count * lax.axis_size("tp"), local_experts * slot_total).astype(
            jnp.bfloat16
        ),
        "tp",
        scatter_dimension=0,
        tiled=True,
    )
    result = summed.reshape(col_count, local_experts, ep_count, capacity)
    returned = lax.all_to_all(result, "ep", split_axis=2, concat_axis=1, tiled=True)
    returned = returned.reshape(col_count, expert_count * capacity)
    picked = (
        jnp.take(returned, slot_index, axis=1)
        .reshape(col_count, row_count, TOP_K)
        .astype(jnp.float32)
    )
    combined = jnp.sum(picked * route_weights[None, :, :], axis=2)
    return combined.T.astype(jnp.bfloat16)


def local(
    query_proj,
    key_proj,
    value_proj,
    sink_logit,
    out_weight,
    expert_input,
    norm_gain,
    routes,
    route_weights,
    gate_weight,
    up_weight,
    down_weight,
):
    mixer_out = mixer_half(query_proj, key_proj, value_proj, sink_logit, out_weight)
    expert_out = expert_half(
        expert_input, norm_gain, routes, route_weights, gate_weight, up_weight, down_weight
    )
    return (mixer_out, expert_out)


def fits_fused(mesh):
    return (
        mesh.shape["tp"] == 4
        and mesh.shape["ep"] == 2 * GROUPS
        and HALF_WIN == SIDE
        and HEADS // KV_HEADS == 4
        and KV_HEADS == 4
    )


class Slots:
    def __init__(self):
        self.names = {}

    def __call__(self, *name):
        return self.names.setdefault(name, len(self.names))


RECV_SLOTS = 40
SEND_SLOTS = 14


def fused_kernel(
    x_hbm, routes_hbm, rw_hbm, gain_hbm, key_hbm, value_hbm, q_hbm, table_hbm, sink_hbm,
    wg_hbm, wu_hbm, wd_hbm, wout_hbm,
    mixer_ref, expert_ref,
    x_ref, routes_ref, rw_ref, gain_ref, key_ref, value_ref, q_ref, table_ref, sink_ref,
    wg, wu, wd, wout,
    kve, krot, att, sel_ret, snd, xs, wgt, hid, yb, yr, zs, rx, ry, sb, r2, fin, ret, acc,
    ssem, rsem, wsem,
):
    ep = lax.axis_index("ep")
    t = lax.axis_index("tp")
    chips = GROUPS
    z, core = ep // 2, ep % 2
    partner = ep + 1 - 2 * core
    other = (ep + 2 * core - 1 + 2 * chips) % (2 * chips)
    up, down = (ep + 1) % (2 * chips), (ep + 2 * chips - 1) % (2 * chips)
    ty, tx = t // 2, t % 2
    t_x, t_y, t_d = ty * 2 + 1 - tx, (1 - ty) * 2 + tx, (1 - ty) * 2 + 1 - tx
    rows = q_ref.shape[0]
    tokens, model = x_ref.shape
    cap = xs.shape[1] // 2
    part = cap // 4
    half_part, half_cap = part // 2, cap // 2
    hidden = wg.shape[1]
    cols = wout.shape[1]
    slots, send_slots = Slots(), Slots()
    z_of = (z, z + 1 - 2 * (z % 2), (z + 2) % chips, chips - 1 - z)

    def remote(send_index, recv_index, src, dst, device):
        return pltpu.make_async_remote_copy(
            src_ref=src, dst_ref=dst, send_sem=ssem.at[send_index], recv_sem=rsem.at[recv_index],
            device_id=device, device_id_type=MESH,
        )

    def send(family, name, src, dst, device):
        remote(send_slots(family), slots(*name), src, dst, device).start()

    def arrive(name, dst):
        remote(0, slots(*name), dst, dst, (ep, t_x)).wait_recv()

    def sent(family, src):
        remote(send_slots(family), 0, src, src, (ep, t_x)).wait_send()

    barrier = pltpu.get_barrier_semaphore()
    peers = [(z_of[k] * 2 + core, t) for k in range(1, chips)]
    peers += [(ep, t_x), (ep, t_y), (partner, t), (other, t)]
    for peer in peers:
        pl.semaphore_signal(barrier, inc=1, device_id=peer, device_id_type=MESH)

    pairs = (
        (x_hbm, x_ref), (routes_hbm, routes_ref), (rw_hbm, rw_ref), (gain_hbm, gain_ref),
        (key_hbm, key_ref), (value_hbm, value_ref), (q_hbm, q_ref), (table_hbm, table_ref),
        (sink_hbm, sink_ref), (wg_hbm, wg), (wu_hbm, wu), (wd_hbm, wd), (wout_hbm, wout),
    )
    order = (0, 1, 2, 3, 4, 4, 4, 5, 6, 7, 8, 9, 10)
    loads = [pltpu.make_async_copy(a, b, wsem.at[i]) for i, (a, b) in zip(order, pairs)]
    for copy in loads[:9]:
        copy.start()
    for copy in loads[:4]:
        copy.wait()
    for copy in loads[9:]:
        copy.start()

    wide = x_ref[...].astype(jnp.float32)
    inverse = lax.rsqrt(jnp.mean(wide * wide, axis=1, keepdims=True) + NORM_EPS)
    normed = (wide * inverse * gain_ref[...]).astype(jnp.bfloat16)
    group = routes_ref[0:1, :] >> 1
    row_i = lax.broadcasted_iota(jnp.int32, (tokens, tokens), 0)
    col_i = lax.broadcasted_iota(jnp.int32, (tokens, tokens), 1)
    later = jnp.where(row_i < col_i, 1.0, 0.0).astype(jnp.bfloat16)
    hot = jnp.where(lax.broadcasted_iota(jnp.int32, (16, tokens), 0) == group, 1.0, 0.0)
    count = jnp.dot(hot.astype(jnp.bfloat16), later, preferred_element_type=jnp.float32)
    rank = jnp.sum(count * hot, axis=0, keepdims=True).astype(jnp.int32)

    odd = (routes_ref[...] & 1) == 1
    weight_odd = jnp.sum(jnp.where(odd, rw_ref[...], 0.0), axis=0, keepdims=True)
    weight_even = jnp.sum(jnp.where(odd, 0.0, rw_ref[...]), axis=0, keepdims=True)
    lane = lax.broadcasted_iota(jnp.int32, (128, tokens), 0)
    weight = jnp.where(lane < 2, weight_even, weight_odd)
    high = weight.astype(jnp.bfloat16).astype(jnp.float32)
    weight = jnp.where((lane & 1) == 0, high, weight - high)
    weight = jnp.where(lane < 4, weight, 0.0).astype(jnp.bfloat16)

    def select(pick, out, at):
        pick = jnp.where(pick, 1.0, 0.0).astype(jnp.bfloat16)
        out[at, model:] = lax.dot_general(
            pick, weight, (((1,), (1,)), ((), ())), preferred_element_type=jnp.float32
        ).astype(jnp.bfloat16)
        out[at, :model] = jnp.dot(pick, normed, preferred_element_type=jnp.float32).astype(
            jnp.bfloat16
        )

    def group_at(index):
        return jnp.where(
            index == 0, z_of[0],
            jnp.where(index == 1, z_of[1], jnp.where(index == 2, z_of[2], z_of[3])),
        )

    pieces = ((1, t, "z"), (2, t, "z"), (1, t_d, "s"), (3, t, "z"), (3, t_d, "s"))
    slot = lax.broadcasted_iota(jnp.int32, (len(pieces) * part, tokens), 0)
    index = slot // part
    owner = jnp.where((index == 2) | (index == 4), t_d, t)
    step = jnp.where(index == 1, 2, jnp.where(index >= 3, 3, 1))
    select(
        (group == group_at(step)) & (rank == owner * part + lax.rem(slot, part)), snd,
        slice(0, len(pieces) * part),
    )

    def piece(k, owner_t, start=0, count=part):
        first = pl.multiple_of(core * cap + owner_t * part + start, 16)
        return xs.at[k, pl.ds(first, count)]

    def own_rows(k, which):
        return xs.at[k, pl.ds(pl.multiple_of(which * cap, 16), cap)]

    pltpu.make_async_copy(att.at[pl.ds(0, 3)], att.at[pl.ds(0, 3)], wsem.at[4]).wait()
    for copy in loads[7:9]:
        copy.wait()
    row_i = lax.broadcasted_iota(jnp.int32, (key_ref.shape[1], 2 * HEAD_DIM), 0)
    col_i = lax.broadcasted_iota(jnp.int32, (key_ref.shape[1], 2 * HEAD_DIM), 1)
    own_key = jnp.where((row_i == t * HEAD_DIM + col_i) & (col_i < HEAD_DIM), 1.0, 0.0)
    own_value = jnp.where(
        (row_i == (t - 1) * HEAD_DIM + col_i) & (col_i >= HEAD_DIM), 1.0, 0.0
    )
    both = jnp.dot(
        key_ref[...], own_key.astype(jnp.bfloat16), preferred_element_type=jnp.float32
    ) + jnp.dot(
        value_ref[...], own_value.astype(jnp.bfloat16), preferred_element_type=jnp.float32
    )
    kve[SIDE : SIDE + rows, :] = both.astype(jnp.bfloat16)

    pl.semaphore_wait(barrier, len(peers))
    send("halo", ("halo",), kve.at[pl.ds(rows, SIDE)], kve.at[pl.ds(0, SIDE)], (up, t))
    send("halo", ("halo",), kve.at[pl.ds(SIDE, SIDE)], kve.at[pl.ds(SIDE + rows, SIDE)], (down, t))
    def dispatch(i):
        k, owner_t, name = pieces[i]
        send(
            "z", (name, k), snd.at[pl.ds(i * part, part)], piece(k, owner_t),
            (z_of[k] * 2 + core, t),
        )

    dispatch(0)

    slot = lax.broadcasted_iota(jnp.int32, (cap, tokens), 0)
    select(
        (group == z) & (rank == slot), xs.at[0], pl.ds(pl.multiple_of(core * cap, 16), cap)
    )
    send("p", ("p", 0), own_rows(0, core), own_rows(0, core), (partner, t))

    def select_back():
        slot = lax.broadcasted_iota(jnp.int32, (chips * cap, tokens), 0)
        place = (group == group_at(slot // cap)) & (rank == lax.rem(slot, cap))
        sel_ret[...] = jnp.where(place, 1.0, 0.0).T.astype(jnp.bfloat16)

    def spread(k):
        arrive(("z", k), piece(k, t))
        if k != 2:
            send("x", ("s", k), piece(k, t), piece(k, t), (ep, t_x))
            send("y", ("s", k), piece(k, t), piece(k, t), (ep, t_y))
            return
        for family, name, start, device in (
            ("x", "xl", 0, t_x), ("y", "yh", half_part, t_y),
            ("x", "s", half_part, t_x), ("y", "s", 0, t_y),
        ):
            rows_of = piece(k, t, start, half_part)
            send(family, (name, k), rows_of, rows_of, (ep, device))

    def relay(k, half):
        name, source, target = (("xl", t_x, t_y), ("yh", t_y, t_x))[half]
        rows_of = piece(k, source, half * half_part, half_part)
        arrive((name, k), rows_of)
        send("d", ("s", k), rows_of, rows_of, (ep, target))

    def share(k):
        arrive(("s", k), snd.at[pl.ds(0, (2 if k == 2 else 3) * part)])
        send("p", ("p", k), own_rows(k, core), own_rows(k, core), (partner, t))

    def swap_matrix(size):
        i = lax.broadcasted_iota(jnp.int32, (size, size), 0)
        j = lax.broadcasted_iota(jnp.int32, (size, size), 1)
        half = HEAD_DIM // 2
        low = (j & (HEAD_DIM - 1)) < half
        minus = low & (i == j + half)
        plus = (~low) & (i == j - half)
        return jnp.where(minus, -1.0, jnp.where(plus, 1.0, 0.0)).astype(jnp.bfloat16)

    blocks = rows // SIDE
    far_rows = (table_ref.shape[0] - 2 * SIDE) // 2

    def tables(block):
        at = ep * blocks + block
        far_c = table_ref[pl.ds(at, 1), :]
        far_s = table_ref[pl.ds(far_rows + at, 1), :]
        near_c = table_ref[2 * far_rows : 2 * far_rows + SIDE, :]
        near_s = table_ref[2 * far_rows + SIDE :, :]
        return far_c * near_c - far_s * near_s, far_s * near_c + far_c * near_s

    def rotate_keys(which):
        swap = swap_matrix(2 * HEAD_DIM)
        for block in which:
            cosine, sine = tables(block)
            raw = kve[block * SIDE : (block + 1) * SIDE, :]
            turned = jnp.dot(raw, swap, preferred_element_type=jnp.float32)
            krot[block * SIDE : (block + 1) * SIDE, :] = (
                raw.astype(jnp.float32) * cosine + turned * sine
            ).astype(jnp.bfloat16)

    heads = HEADS // KV_HEADS

    def attend(block):
        swap = swap_matrix(heads * HEAD_DIM)
        cosine, sine = tables(block + 1)
        cosine = jnp.concatenate([cosine] * (heads // 2), axis=1)
        sine = jnp.concatenate([sine] * (heads // 2), axis=1)
        raw = q_ref[block * SIDE : (block + 1) * SIDE, :]
        turned = jnp.dot(raw, swap, preferred_element_type=jnp.float32)
        query = (
            (raw.astype(jnp.float32) * cosine + turned * sine) * HEAD_DIM ** (-0.5)
        ).astype(jnp.bfloat16)
        query = jnp.concatenate(
            [query[:, h * HEAD_DIM : (h + 1) * HEAD_DIM] for h in range(heads)], axis=0
        )
        span = 3 * SIDE
        keys = krot[block * SIDE : block * SIDE + span, :HEAD_DIM]
        values = kve[block * SIDE : block * SIDE + span, HEAD_DIM:]
        scores = lax.dot_general(
            query, keys, (((1,), (1,)), ((), ())), preferred_element_type=jnp.float32
        )
        row = lax.broadcasted_iota(jnp.int32, scores.shape, 0) & (SIDE - 1)
        col = lax.broadcasted_iota(jnp.int32, scores.shape, 1)
        gap = col - row
        absolute = col + (ep * rows + (block - 1) * SIDE)
        allowed = (gap >= 0) & (gap <= 2 * HALF_WIN)
        allowed = allowed & (absolute >= 0) & (absolute < rows * 2 * chips)
        scores = jnp.where(allowed, scores, NEG_BIG)
        head = lax.broadcasted_iota(jnp.int32, (heads * SIDE, 1), 0) // SIDE
        sink = jnp.zeros((heads * SIDE, 1), jnp.float32)
        for h in range(heads):
            sink = jnp.where(head == h, sink_ref[h], sink)
        peak = jnp.maximum(jnp.max(scores, axis=1, keepdims=True), sink)
        lifted = jnp.exp(scores - peak)
        total = jnp.sum(lifted, axis=1, keepdims=True) + jnp.exp(sink - peak)
        out = jnp.dot(lifted.astype(jnp.bfloat16), values, preferred_element_type=jnp.float32)
        out = (out / total).astype(jnp.bfloat16)
        att[t, block * SIDE : (block + 1) * SIDE, :] = jnp.concatenate(
            [out[h * SIDE : (h + 1) * SIDE, :] for h in range(heads)], axis=1
        )

    def edges():
        arrive(("halo",), kve.at[pl.ds(0, 2 * SIDE)])
        rotate_keys((0, blocks + 1))

    tile = 256

    def gather(k):
        arrive(("p", k), own_rows(k, 1 - core))
        tag = xs[k, :, model:].astype(jnp.float32)
        lane = lax.broadcasted_iota(jnp.int32, tag.shape, 1)
        weight = jnp.sum(jnp.where(lane // 2 == core, tag, 0.0), axis=1, keepdims=True)
        wgt[...] = jnp.broadcast_to(weight, wgt.shape)

    def widen(k, start, stop):
        for i in range(start, stop):
            at = pl.ds(i * tile, tile)
            gate = jnp.dot(xs[k, :, :model], wg[:, at], preferred_element_type=jnp.float32)
            lift = jnp.dot(xs[k, :, :model], wu[:, at], preferred_element_type=jnp.float32)
            value = gate / (1.0 + jnp.exp(-gate)) * lift
            weight = jnp.concatenate([wgt[...]] * (tile // wgt.shape[1]), axis=1)
            hid[:, at] = (value * weight).astype(jnp.bfloat16)

    last = chips - 1

    def target_of(i):
        return (t_d, t_y, t_x, t)[i]

    def narrow(k, *chunks):
        theirs = pl.ds(pl.multiple_of((1 - core) * cap, 16), cap)
        for i in chunks:
            target = target_of(i)
            at = pl.ds(pl.multiple_of(target * cols, cols), cols)
            yb[k, target] = jnp.dot(
                hid[...], wd[:, at], preferred_element_type=jnp.float32
            ).astype(jnp.bfloat16)
        for i in chunks:
            target = target_of(i)
            name = ("q", k, i) if k >= 2 else ("q", k)
            send("q", name, yb.at[k, target, theirs], yr.at[k, target], (partner, t))

    def add(*parts):
        return sum(p.astype(jnp.float32) for p in parts).astype(jnp.bfloat16)

    first, second = slice(0, half_cap), slice(half_cap, cap)
    d_first, d_second = pl.ds(0, half_cap), pl.ds(half_cap, half_cap)

    def scatter_add(k, i):
        target = target_of(i)
        if k >= 2:
            arrive(("q", k, i), yr.at[k, target])
        elif i == 0:
            arrive(("q", k), yr.at[k])
        mine = pl.ds(pl.multiple_of(core * cap, 16), cap)
        zs[k, target] = add(yb[k, target, mine], yr[k, target])

    def scatter_send(k, i):
        if i == 0:
            send("rx", ("rx", k), zs.at[k, t_d, d_first], rx.at[k, 1], (ep, t_x))
            send("ry", ("ry", k), zs.at[k, t_d, d_second], ry.at[k, 1], (ep, t_y))
        if i == 1:
            send("ry", ("g", k), zs.at[k, t_y, d_second], ry.at[k, 0], (ep, t_y))
        if i == 2:
            send("rx", ("g", k), zs.at[k, t_x, d_first], rx.at[k, 0], (ep, t_x))

    def scatter_one(k, i):
        scatter_add(k, i)
        scatter_send(k, i)

    def scatter_two(k):
        arrive(("rx", k), rx.at[k, 1])
        sb[k, 0] = add(zs[k, t_y, first], rx[k, 1])
        send("r2", ("g", k), sb.at[k, 0], r2.at[k, 0], (ep, t_y))
        arrive(("ry", k), ry.at[k, 1])
        sb[k, 1] = add(zs[k, t_x, second], ry[k, 1])
        send("r2", ("g", k), sb.at[k, 1], r2.at[k, 1], (ep, t_x))

    def give_back(k):
        arrive(("g", k), r2.at[pl.ds(0, 2)])
        target = fin if k else ret
        target[k, first] = add(zs[k, t, first], rx[k, 0], r2[k, 0])
        target[k, second] = add(zs[k, t, second], ry[k, 0], r2[k, 1])
        if k:
            name = ("ret", last) if k == last else ("ret",)
            send("ret", name, fin.at[k], ret.at[k], (z_of[k] * 2 + core, t))

    def wait_back_early():
        arrive(("ret",), ret.at[pl.ds(1, last - 1)])

    def wait_back():
        arrive(("ret", last), ret.at[last])

    mid = pl.ds(SIDE, rows - 2 * SIDE)
    ends = (pl.ds(0, SIDE), pl.ds(rows - SIDE, SIDE))

    def attended_mid():
        send("ax", ("axm",), att.at[t, mid], att.at[t, mid], (ep, t_x))
        send("ay", ("proj",), att.at[t, mid], att.at[t, mid], (ep, t_y))

    def attended_ends():
        for at in ends:
            send("ay", ("aye",), att.at[t, at], att.at[t, at], (ep, t_y))
            send("ax", ("proj",), att.at[t, at], att.at[t, at], (ep, t_x))

    def attended_relay_mid():
        arrive(("axm",), att.at[t_x, mid])
        send("ad", ("proj",), att.at[t_x, mid], att.at[t_x, mid], (ep, t_y))

    def attended_relay_ends():
        arrive(("aye",), att.at[t_y, pl.ds(0, 2 * SIDE)])
        for at in ends:
            send("ad", ("proj",), att.at[t_y, at], att.at[t_y, at], (ep, t_x))

    def project():
        arrive(("proj",), att.at[pl.ds(0, 2)])
        width = att.shape[2]
        total = jnp.zeros((rows, cols), jnp.float32)
        for i in range(4):
            total += jnp.dot(
                att[i], wout[i * width : (i + 1) * width, :], preferred_element_type=jnp.float32
            )
        mixer_ref[...] = total.astype(jnp.bfloat16)

    def load_wait(i):
        loads[9 + i].wait()

    def place_early():
        count = (chips - 1) * cap
        acc[...] = jnp.dot(
            sel_ret[:, :count], ret[: chips - 1].reshape(count, cols),
            preferred_element_type=jnp.float32,
        )

    def place_last():
        count = (chips - 1) * cap
        expert_ref[...] = (
            acc[...]
            + jnp.dot(sel_ret[:, count:], ret[chips - 1], preferred_element_type=jnp.float32)
        ).astype(jnp.bfloat16)

    rotate_keys(range(1, blocks + 1))
    attend(1)
    dispatch(1)
    dispatch(2)
    attend(2)
    attended_mid()
    dispatch(3)
    edges()
    attend(0)
    attend(3)
    attended_ends()
    load_wait(0)
    load_wait(1)
    gather(0)
    widen(0, 0, 2)
    spread(1)
    widen(0, 2, 4)
    load_wait(2)
    narrow(0, 0, 1, 2, 3)
    spread(2)
    dispatch(4)
    select_back()
    share(1)
    relay(2, 0)
    scatter_add(0, 0)
    scatter_add(0, 1)
    scatter_add(0, 2)
    scatter_add(0, 3)
    gather(1)
    relay(2, 1)
    widen(1, 0, 2)
    attended_relay_mid()
    attended_relay_ends()
    widen(1, 2, 4)
    narrow(1, 0)
    spread(3)
    narrow(1, 1, 2)
    share(2)
    narrow(1, 3)
    gather(2)
    widen(2, 0, 1)
    scatter_one(1, 0)
    scatter_one(1, 1)
    scatter_one(1, 2)
    scatter_one(1, 3)
    widen(2, 1, 4)
    narrow(2, 0, 1)
    share(3)
    scatter_one(2, 0)
    narrow(2, 2)
    scatter_one(2, 1)
    narrow(2, 3)
    scatter_one(2, 2)
    gather(3)
    widen(3, 0, 1)
    scatter_one(2, 3)
    scatter_two(1)
    widen(3, 1, 4)
    narrow(3, 0, 1)
    scatter_two(2)
    narrow(3, 2)
    scatter_one(3, 0)
    narrow(3, 3)
    scatter_one(3, 1)
    scatter_one(3, 2)
    scatter_one(3, 3)
    give_back(1)
    load_wait(3)
    project()
    give_back(2)
    scatter_two(3)
    scatter_send(0, 0)
    scatter_send(0, 1)
    scatter_send(0, 2)
    give_back(3)
    scatter_two(0)
    give_back(0)
    wait_back_early()
    place_early()
    wait_back()
    place_last()
    for family, ref in (
        ("halo", kve.at[pl.ds(0, 2 * SIDE)]), ("z", snd), ("p", xs.at[:, pl.ds(0, cap)]),
        ("x", snd.at[pl.ds(0, 3 * part)]), ("y", snd.at[pl.ds(0, 3 * part)]),
        ("d", snd.at[pl.ds(0, part)]), ("q", yr), ("rx", rx), ("ry", ry), ("r2", r2),
        ("ret", fin.at[pl.ds(1, last)]), ("ax", att.at[0]), ("ay", att.at[0]),
        ("ad", att.at[0]),
    ):
        sent(family, ref)


def local_fused(
    query_proj, key_proj, value_proj, sink_logit, out_weight, expert_input, norm_gain,
    routes, route_weights, gate_weight, up_weight, down_weight,
):
    rows = query_proj.shape[0]
    tokens, model = expert_input.shape
    cols = out_weight.shape[1]
    hidden = gate_weight.shape[2]
    cap = tokens // 2
    bf16, f32 = jnp.bfloat16, jnp.float32
    half = HEAD_DIM // 2
    channel = np.arange(2 * HEAD_DIM) % half
    inverse_freq = 1.0 / ROPE_BASE ** (channel * 2.0 / HEAD_DIM)
    far_count = -(-(lax.axis_size("ep") * (rows // SIDE) + 2) // 8) * 8
    far = (np.arange(far_count) - 1)[:, None] * SIDE * inverse_freq[None, :]
    near = np.arange(SIDE)[:, None] * inverse_freq[None, :]
    table = np.concatenate([np.cos(far), np.sin(far), np.cos(near), np.sin(near)]).astype(
        np.float32
    )
    hbm = pl.BlockSpec(memory_space=pltpu.HBM)
    vmem = pl.BlockSpec(memory_space=pltpu.VMEM)
    args = (
        expert_input, routes.T, route_weights.T, norm_gain[None, :], key_proj, value_proj,
        query_proj, jnp.asarray(table), sink_logit, gate_weight[0], up_weight[0], down_weight[0],
        out_weight,
    )
    scratch = [
        (pltpu.SMEM if a is sink_logit else pltpu.VMEM)(a.shape, a.dtype) for a in args
    ] + [
        pltpu.VMEM((rows + 2 * SIDE, 2 * HEAD_DIM), bf16),
        pltpu.VMEM((rows + 2 * SIDE, 2 * HEAD_DIM), bf16),
        pltpu.VMEM((4, rows, query_proj.shape[1]), bf16),
        pltpu.VMEM((tokens, GROUPS * cap), bf16),
        pltpu.VMEM((5 * cap // 4, model + 128), bf16),
        pltpu.VMEM((GROUPS, 2 * cap, model + 128), bf16),
        pltpu.VMEM((2 * cap, 128), f32),
        pltpu.VMEM((2 * cap, hidden), bf16),
        pltpu.VMEM((GROUPS, 4, 2 * cap, cols), bf16),
        pltpu.VMEM((GROUPS, 4, cap, cols), bf16),
        pltpu.VMEM((GROUPS, 4, cap, cols), bf16),
        pltpu.VMEM((GROUPS, 2, cap // 2, cols), bf16),
        pltpu.VMEM((GROUPS, 2, cap // 2, cols), bf16),
        pltpu.VMEM((GROUPS, 2, cap // 2, cols), bf16),
        pltpu.VMEM((GROUPS, 2, cap // 2, cols), bf16),
        pltpu.VMEM((GROUPS, cap, cols), bf16),
        pltpu.VMEM((GROUPS, cap, cols), bf16),
        pltpu.VMEM((tokens, cols), f32),
        pltpu.SemaphoreType.DMA((SEND_SLOTS,)),
        pltpu.SemaphoreType.DMA((RECV_SLOTS,)),
        pltpu.SemaphoreType.DMA((len(args) - 2,)),
    ]
    return pl.pallas_call(
        fused_kernel,
        out_shape=(pltpu.VMEM((rows, cols), bf16), pltpu.VMEM((tokens, cols), bf16)),
        in_specs=[hbm] * len(args),
        out_specs=(vmem, vmem),
        scratch_shapes=scratch,
        compiler_params=pltpu.CompilerParams(
            collective_id=0, has_side_effects=True, vmem_limit_bytes=60 * 1024 * 1024
        ),
    )(*args)


def solution(mesh):
    fused = fits_fused(mesh)
    return jax.shard_map(
        local_fused if fused else local,
        mesh=mesh,
        in_specs=(
            P("ep", "tp"),
            P("ep", None),
            P("ep", None),
            P("tp"),
            P(None, "tp"),
            P("ep", None),
            P(),
            P("ep", None),
            P("ep", None),
            P("ep", None, "tp"),
            P("ep", None, "tp"),
            P("ep", "tp", None),
        ),
        out_specs=(P("ep", "tp"), P("ep", "tp")),
        check_vma=False,
    )
```
